128 devices in a mesh: sp: 16 (over z, y), dp: 8 (over x, core).
Axes of the slice: x: 4, y: 4, z: 4, core: 2. Of those that a mesh axis runs over, the one named last changes fastest.
Arguments:
- out_cotangent: bfloat16 [8, 4096, 2048], P('dp', 'sp'), may hold values from -6 to 6
- value_pre: bfloat16 [8, 4096, 2048], P('dp', 'sp'), may hold values from -8 to 8
- gate_pre: bfloat16 [8, 4096, 2048], P('dp', 'sp'), may hold values from -8 to 8
- out_weight: bfloat16 [2048, 2048], P('dp'), may hold values from -0.125 to 0.125
- conv_kernel: bfloat16 [31, 2048], P(None, 'sp'), may hold values from -6 to 6
- norm_gain: bfloat16 [2048], P('sp'), may hold values from 0.099609375 to 1.8984375
Outputs:
- grad_value: bfloat16 [8, 4096, 2048], P('dp', 'sp')
- grad_gate: bfloat16 [8, 4096, 2048], P('dp', 'sp')
- grad_out_weight: float32 [2048, 2048], P(('sp', 'dp'))
- grad_kernel: float32 [31, 2048], P(None, 'sp')
- grad_gain: float32 [2048], P('sp')
The draws below stay inside these ranges and needn't reach their ends.
All inputs are finite; a program needn't handle non-finite values.
Results may differ from the reference program's by a relative error of at most 0.011.
Values may be sent and summed in bfloat16 or wider, within the bound.
A program may use at most 128 MiB of HBM per device.

```python
import math
import jax
import jax.numpy as jnp
from jax import lax

D = 2048
CONV_W = 31
SEQS = 8
LENGTH = 4096
TOKENS = 32768


def draw_value_pre(key, part):
    keys = jax.random.split(jax.random.fold_in(key, 11), 2)
    shape = (SEQS, LENGTH, D)
    row_scale = jnp.exp(jax.random.uniform(keys[1], (SEQS, LENGTH, 1), jnp.float32, math.log(0.4), math.log(2.5)))
    values_out = jax.random.normal(keys[0], shape, jnp.float32) * row_scale
    return jnp.clip(values_out, -8.0, 8.0).astype(jnp.bfloat16)


def draw_conv_kernel(key, part):
    keys = jax.random.split(jax.random.fold_in(key, 23), 2)
    position = jnp.arange(D, dtype=jnp.float32) / float(D)
    rough = jnp.exp(jax.random.uniform(keys[1], (1, D), jnp.float32, math.log(0.5), math.log(2.0)))
    column_scale = jnp.exp(math.log(6.0) * position)[None, :] * rough
    taps = jax.random.normal(keys[0], (CONV_W, D), jnp.float32)
    taps = taps * column_scale * float(CONV_W) ** (-0.5)
    return jnp.clip(taps, -6.0, 6.0).astype(jnp.bfloat16)


def shard_levels(rng, shape, pieces, low, high):
    def one(axis_at, blocks):
        steps = jax.random.uniform(jax.random.fold_in(jax.random.fold_in(rng, 6), axis_at), (blocks,), jnp.float32, low / len(pieces), high / len(pieces))
        return jnp.repeat(jnp.exp(steps), shape[axis_at] // blocks).reshape((-1,) + (1,) * (len(shape) - axis_at - 1))

    gain = one(*pieces[0])
    for cut in pieces[1:]:
        gain = gain * one(*cut)
    return gain


def normal_values(rng, shape, spread, limit, cuts=(), kind=jnp.bfloat16):
    values = jax.random.normal(rng, shape, jnp.float32) * spread
    if len(cuts) > 0:
        values = shard_levels(rng, shape, cuts, -0.22, 0.18) * values
    return jnp.clip(values, min=-limit, max=limit).astype(kind)


def setup_inputs(seed: int = 0) -> dict:
    key_list = jax.random.split(jax.random.key(seed), 7)
    out_cotangent = normal_values(key_list[0], (SEQS, LENGTH, D), 1.0, 6.0, ((0, 8), (1, 16)))
    value_pre = draw_value_pre(jax.random.fold_in(key_list[6], 71), 0)
    gate_pre = normal_values(key_list[2], (SEQS, LENGTH, D), 1.5, 8.0, ((0, 8), (1, 16)))
    out_weight = normal_values(key_list[3], (D, D), D ** -0.5, 0.125, ((0, 8),))
    conv_kernel = draw_conv_kernel(jax.random.fold_in(key_list[6], 71), 0)
    norm_gain = jnp.clip(1.0 + 0.18 * jax.random.normal(key_list[5], (D,), jnp.float32), 0.099609375, 1.8984375).astype(jnp.bfloat16)
    return {"out_cotangent": out_cotangent, "value_pre": value_pre, "gate_pre": gate_pre, "out_weight": out_weight, "conv_kernel": conv_kernel, "norm_gain": norm_gain}


epsilon = 1e-05

def shift_down(array, offset):
    return jnp.pad(array, ((offset, 0), (0, 0)))[:array.shape[0]]

def shift_up(array, offset):
    return jnp.pad(array, ((0, offset), (0, 0)))[offset:]

def reference(out_cotangent, value_pre, gate_pre, out_weight, conv_kernel, norm_gain):
    taps_float = conv_kernel.astype(jnp.float32)
    gain_float = norm_gain.astype(jnp.float32)
    weight_sum = jnp.zeros((D, D), jnp.float32)
    kernel_sum = jnp.zeros((CONV_W, D), jnp.float32)
    gain_sum = jnp.zeros((D,), jnp.float32)
    value_grads = []
    gate_grads = []
    for sequence in range(SEQS):
        cotangent = out_cotangent[sequence]
        values_in = value_pre[sequence].astype(jnp.float32)
        sigmoid_gate = jax.nn.sigmoid(gate_pre[sequence].astype(jnp.float32))
        gated = (values_in * sigmoid_gate).astype(jnp.bfloat16)
        gated_float = gated.astype(jnp.float32)
        conv = jnp.zeros(gated_float.shape, jnp.float32)
        for offset in range(CONV_W):
            conv = conv + taps_float[offset] * shift_down(gated_float, offset)
        centre = lax.optimization_barrier(jnp.mean(conv, axis=1, keepdims=True))
        deviation = conv - centre
        variance = lax.optimization_barrier(jnp.mean(deviation * deviation, axis=1, keepdims=True))
        inv_scale = lax.rsqrt(variance + epsilon)
        centred = deviation * inv_scale
        normed = centred * gain_float
        activation = jax.nn.silu(normed).astype(jnp.bfloat16)
        grad_act = lax.dot_general(cotangent, out_weight, (((1,), (1,)), ((), ())), preferred_element_type=jnp.float32).astype(jnp.bfloat16)
        weight_sum = weight_sum + lax.dot_general(activation, cotangent, (((0,), (0,)), ((), ())), preferred_element_type=jnp.float32)
        sig_norm = jax.nn.sigmoid(normed)
        grad_normed = grad_act.astype(jnp.float32) * sig_norm * (1.0 + normed * (1.0 - sig_norm))
        gain_sum = gain_sum + lax.optimization_barrier(jnp.sum(grad_normed * centred, axis=0))
        grad_centred = grad_normed * gain_float
        grad_conv = (grad_centred - lax.optimization_barrier(jnp.mean(grad_centred, axis=1, keepdims=True)) - centred * lax.optimization_barrier(jnp.mean(grad_centred * centred, axis=1, keepdims=True))) * inv_scale
        kernel_rows = [lax.optimization_barrier(jnp.sum(grad_conv * shift_down(gated_float, offset), axis=0)) for offset in range(CONV_W)]
        kernel_sum = kernel_sum + jnp.stack(kernel_rows, axis=0)
        grad_gated = jnp.zeros(grad_conv.shape, jnp.float32)
        for offset in range(CONV_W):
            grad_gated = grad_gated + taps_float[offset] * shift_up(grad_conv, offset)
        grad_gated = grad_gated.astype(jnp.bfloat16).astype(jnp.float32)
        value_grads.append((grad_gated * sigmoid_gate).astype(jnp.bfloat16))
        gate_grads.append((grad_gated * values_in * sigmoid_gate * (1.0 - sigmoid_gate)).astype(jnp.bfloat16))
    factor = float(TOKENS) ** (-0.5)
    return (jnp.stack(value_grads, axis=0), jnp.stack(gate_grads, axis=0), weight_sum * factor, kernel_sum * factor, gain_sum * factor)
```

```python
import functools

import jax
import jax.numpy as jnp
from jax import lax
from jax.experimental import pallas as pl
from jax.experimental.pallas import tpu as pltpu
from jax.sharding import PartitionSpec as P

EPS = 1e-05
F32 = jnp.float32
BF16 = jnp.bfloat16
MESH = pl.DeviceIdType.MESH

ROWS = 256
SEG = 32
D = 2048
HALF = 1024
TAPS = 31
NSP = 16
NDP = 8
COLOURS = ((0, 384), (384, 384), (768, 256))

TAP0 = 0
COT0 = TAP0 + 16
HALO0 = COT0 + 1
WX0 = HALO0 + 1
WY0 = WX0 + 8
WZ0 = WY0 + 12
ACT0 = WZ0 + 12
GA0 = ACT0 + 4
RA0 = GA0 + 4
RB0 = RA0 + 18
RC0 = RB0 + 9
GK0 = RC0 + 9
GD0 = GK0 + 16
GC0 = GD0 + 8
FIN0 = GC0 + 1
NSEM = FIN0 + 1


def sigmoid(x):
    return 0.5 * jnp.tanh(0.5 * x) + 0.5


def lanes(i, n=128):
    return pl.ds(pl.multiple_of(i * n, n), n)


def rows(i, n):
    return pl.ds(pl.multiple_of(i * n, n), n)


def loop(n, body):
    def step(i, c):
        body(i)
        return c

    lax.fori_loop(0, n, step, 0)


def kernel(
    cot_hbm,
    val_hbm,
    gate_hbm,
    w_hbm,
    taps_in,
    gain_in,
    gv_hbm,
    gg_hbm,
    ow_ref,
    gk_ref,
    cotraw,
    cotp,
    val,
    gate,
    sig,
    gext,
    ext,
    cen,
    fwd,
    act,
    wg,
    ga,
    tkown,
    tkall,
    tkf,
    sum1,
    sum2,
    inv_b,
    hal,
    halr,
    ggp,
    gvo,
    ggo,
    gkp,
    gkr,
    gdo,
    gdr,
    pa,
    pb,
    pc,
    r1a,
    r1b,
    r1c,
    cba,
    cbb,
    cbc,
    s1a,
    s1b,
    s1c,
    r2a,
    r2b,
    r2c,
    s2a,
    s2b,
    s2c,
    r3a,
    r3b,
    r3c,
    finp,
    fins,
    finr,
    perm,
    permt,
    ssem,
    rsem,
    lsem,
):
    s = lax.axis_index("sp")
    d = lax.axis_index("dp")
    z, y = s // 4, s % 4
    x, q = d // 2, d % 2

    def at(axis, off):
        if axis == 0:
            return {"sp": s, "dp": ((x + off) % 4) * 2 + q}
        if axis == 1:
            return {"sp": z * 4 + (y + off) % 4, "dp": d}
        return {"sp": ((z + off) % 4) * 4 + y, "dp": d}

    partner = {"sp": s, "dp": x * 2 + (1 - q)}
    coord = (x, y, z)

    sent = []

    def copy(src, dst, i, dev):
        return pltpu.make_async_remote_copy(
            src_ref=src, dst_ref=dst, send_sem=ssem.at[i], recv_sem=rsem.at[i], device_id=dev, device_id_type=MESH
        )

    def send(src, dst, i, dev):
        c = copy(src, dst, i, dev)
        c.start()
        sent.append(c)

    def got(dst, i):
        copy(dst, dst, i, partner).wait_recv()

    local = [
        pltpu.make_async_copy(w_hbm, wg.at[x], lsem.at[0]),
        pltpu.make_async_copy(val_hbm, val, lsem.at[1]),
        pltpu.make_async_copy(gate_hbm, gate, lsem.at[2]),
        pltpu.make_async_copy(cot_hbm, cotraw.at[q], lsem.at[3]),
    ]
    for c in local:
        c.start()
    barrier = pltpu.get_barrier_semaphore()

    def greet_sp(r):
        pl.semaphore_signal(barrier, inc=1, device_id={"sp": (s + r + 1) % NSP, "dp": d}, device_id_type=MESH)

    def greet_dp(r):
        pl.semaphore_signal(barrier, inc=1, device_id={"sp": s, "dp": (d + r + 1) % NDP}, device_id_type=MESH)

    loop(NSP - 1, greet_sp)
    loop(NDP - 1, greet_dp)
    tkown[0:TAPS, :] = taps_in[...].astype(F32)
    tkown[TAPS : TAPS + 1, :] = gain_in[...].astype(F32)
    tkall[s] = tkown[...].astype(BF16)
    r_io = lax.broadcasted_iota(jnp.int32, (ROWS, ROWS), 0)
    t_io = lax.broadcasted_iota(jnp.int32, (ROWS, ROWS), 1)
    perm[...] = jnp.where(t_io == (r_io & 7) * SEG + (r_io >> 3), 1.0, 0.0).astype(BF16)
    permt[...] = jnp.where(r_io == (t_io & 7) * SEG + (t_io >> 3), 1.0, 0.0).astype(BF16)
    pl.semaphore_wait(barrier, NSP - 1 + NDP - 1)

    def wy(xx, yy, h=None):
        if h is None:
            return wg.at[xx, pl.ds(pl.multiple_of(yy * 64, 64), 64), pl.ds(0, HALF)]
        return wg.at[xx, pl.ds(pl.multiple_of(yy * 64 + h * 32, 32), 32), pl.ds(0, HALF)]

    def wz(xx, zz, h=None):
        if h is None:
            return wg.at[xx, pl.ds(pl.multiple_of(zz * 64, 64), 64), pl.ds(HALF, HALF)]
        return wg.at[xx, pl.ds(pl.multiple_of(zz * 64 + h * 32, 32), 32), pl.ds(HALF, HALF)]

    local[0].wait()
    for i, off in ((0, 1), (1, -1)):
        send(wy(x, y), wy(x, y), WX0 + i, at(0, off))
        send(wz(x, z), wz(x, z), WX0 + 2 + i, at(0, off))

    def send_taps(r):
        copy(tkall.at[s], tkall.at[s], TAP0 + r, {"sp": (s + r + 1) % NSP, "dp": d}).start()

    loop(NSP - 1, send_taps)

    local[1].wait()
    local[2].wait()

    def gate_block(i):
        at_rows = rows(ROWS // 32 - 1 - i, 32)
        sg = sigmoid(gate[at_rows, :].astype(F32))
        sig[at_rows, :] = sg
        gext[pl.ds(pl.multiple_of((ROWS // 32 - i) * 32, 32), 32), :] = (val[at_rows, :].astype(F32) * sg).astype(BF16)

    gate_block(0)

    def halo_copy():
        return copy(gext.at[pl.ds(ROWS, 32)], gext.at[pl.ds(0, 32)], HALO0, {"sp": (s + 1) % NSP, "dp": d})

    @pl.when(s < NSP - 1)
    def _():
        halo_copy().start()

    local[3].wait()
    send(cotraw.at[q], cotraw.at[q], COT0, partner)
    loop(ROWS // 32 - 1, lambda i: gate_block(i + 1))

    def weights_on(xx, pos):
        for i, off in ((0, 1), (1, -1)):
            send(wy(xx, y), wy(xx, y), WY0 + 4 * pos + i, at(1, off))
            send(wz(xx, z), wz(xx, z), WZ0 + 4 * pos + i, at(2, off))

    def weights_far(xx, pos):
        got(wy(xx, (y + 3) % 4), WY0 + 4 * pos)
        send(wy(xx, (y + 3) % 4, 0), wy(xx, (y + 3) % 4, 0), WY0 + 4 * pos + 2, at(1, 1))
        got(wz(xx, (z + 3) % 4), WZ0 + 4 * pos)
        send(wz(xx, (z + 3) % 4, 0), wz(xx, (z + 3) % 4, 0), WZ0 + 4 * pos + 2, at(2, 1))
        got(wy(xx, (y + 1) % 4), WY0 + 4 * pos + 1)
        send(wy(xx, (y + 1) % 4, 1), wy(xx, (y + 1) % 4, 1), WY0 + 4 * pos + 3, at(1, -1))
        got(wz(xx, (z + 1) % 4), WZ0 + 4 * pos + 1)
        send(wz(xx, (z + 1) % 4, 1), wz(xx, (z + 1) % 4, 1), WZ0 + 4 * pos + 3, at(2, -1))

    def weights_end(xx, pos):
        got(wy(xx, (y + 2) % 4, 0), WY0 + 4 * pos + 2)
        got(wz(xx, (z + 2) % 4, 0), WZ0 + 4 * pos + 2)
        got(wy(xx, (y + 2) % 4, 1), WY0 + 4 * pos + 3)
        got(wz(xx, (z + 2) % 4, 1), WZ0 + 4 * pos + 3)

    left, right, far = (x + 3) % 4, (x + 1) % 4, (x + 2) % 4
    got(wy(left, y), WX0)
    send(wy(left, y, 0), wy(left, y, 0), WX0 + 4, at(0, 1))
    got(wy(right, y), WX0 + 1)
    send(wy(right, y, 1), wy(right, y, 1), WX0 + 5, at(0, -1))
    got(wz(left, z), WX0 + 2)
    send(wz(left, z, 0), wz(left, z, 0), WX0 + 6, at(0, 1))
    got(wz(right, z), WX0 + 3)
    send(wz(right, z, 1), wz(right, z, 1), WX0 + 7, at(0, -1))
    weights_on(left, 0)
    weights_on(right, 1)

    def spread(n, first, base):
        block = jnp.dot(perm[...], gext[pl.ds(first, ROWS), lanes(n, 512)], preferred_element_type=F32)
        for i in range(4):
            ext[n * 4 + i, pl.ds(base, ROWS), :] = block[:, 128 * i : 128 * i + 128]

    loop(4, lambda n: spread(n, 32, ROWS))

    def spread_cot(core):
        def body(n):
            block = jnp.dot(perm[...], cotraw[core, :, lanes(n, 512)], preferred_element_type=F32)
            cotp[rows(core, ROWS), lanes(n, 512)] = block.astype(BF16)

        loop(4, body)

    spread_cot(q)

    @pl.when(s > 0)
    def _():
        got(gext.at[pl.ds(0, 32)], HALO0)

    @pl.when(s == 0)
    def _():
        gext[0:32, :] = jnp.zeros((32, D), BF16)

    loop(4, lambda n: spread(n, 0, 0))

    def got_taps(r):
        src = (s + NSP - 1 - r) % NSP
        got(tkall.at[src], TAP0 + r)

    loop(NSP - 1, got_taps)

    def widen(i):
        tkf[:, lanes(i)] = tkall[i].astype(F32)

    loop(NSP, widen)

    sum1[...] = jnp.zeros((ROWS, 128), F32)
    sum2[...] = jnp.zeros((ROWS, 128), F32)

    def conv_block(i):
        col, jb = i // 4, i % 4
        ln = lanes(col)
        window = {
            o: ext[col, pl.ds(pl.multiple_of((jb * 8 + o + SEG) * 8, 8), 8), :] for o in range(1 - TAPS, 8)
        }
        acc = [None] * 8
        for k in range(TAPS):
            w = jnp.broadcast_to(tkf[k : k + 1, ln], (8, 128))
            for o in range(8):
                term = w * window[o - k]
                acc[o] = term if acc[o] is None else acc[o] + term
        for o in range(8):
            at_rows = pl.ds(pl.multiple_of((jb * 8 + o) * 8, 8), 8)
            cen[col, at_rows, :] = acc[o]
            sum1[at_rows, :] += acc[o]
            sum2[at_rows, :] += acc[o] * acc[o]

    loop(32, conv_block)
    got(wy(far, y, 0), WX0 + 4)
    got(wy(far, y, 1), WX0 + 5)
    got(wz(far, z, 0), WX0 + 6)
    got(wz(far, z, 1), WX0 + 7)
    weights_on(far, 2)
    weights_far(left, 0)
    loop(32, lambda i: conv_block(i + 32))
    weights_far(right, 1)

    mean = jnp.sum(sum1[...], axis=1, keepdims=True) * (1.0 / D)
    var = jnp.sum(sum2[...], axis=1, keepdims=True) * (1.0 / D) - mean * mean
    sum1[...] = jnp.broadcast_to(mean, (ROWS, 128))
    inv_b[...] = jnp.broadcast_to(lax.rsqrt(var + EPS), (ROWS, 128))

    def act_block(i):
        col, jb = i // 4, i % 4
        ln, at_rows = lanes(col), rows(jb, 64)
        centred = (cen[col, at_rows, :] - sum1[at_rows, :]) * inv_b[at_rows, :]
        cen[col, at_rows, :] = centred
        normed = centred * tkf[TAPS : TAPS + 1, ln]
        sg = sigmoid(normed)
        a = normed * sg
        act[pl.ds(pl.multiple_of(q * ROWS + jb * 64, 64), 64), ln] = a.astype(BF16)
        fwd[col, at_rows, :] = sg * (1.0 + normed * (1.0 - sg))

    for g in range(4):
        loop(16, lambda i: act_block(i + 16 * g))
        part = act.at[rows(q, ROWS), pl.ds(512 * g, 512)]
        send(part, part, ACT0 + g, partner)

    weights_far(far, 2)
    got(cotraw.at[1 - q], COT0)
    spread_cot(1 - q)

    blocks = (pa, pb, pc)
    half = lanes(q, HALF)

    def outer(cb):
        p = lax.dot_general(
            act[:, lanes(cb, 256)], cotp[:, half], (((0,), (0,)), ((), ())), preferred_element_type=F32
        ).astype(BF16)
        zz, y0 = cb // 2, (cb % 2) * 2
        for i in range(8):
            yy, xx = y0 + i // 4, i % 4
            piece = p[32 * i : 32 * i + 32]
            pa[xx, yy, zz] = piece[:, 0:384]
            pb[yy, zz, xx] = piece[:, 384:768]
            pc[zz, xx, yy] = piece[:, 768:1024]

    for g in range(4):
        got(act.at[rows(1 - q, ROWS), pl.ds(512 * g, 512)], ACT0 + g)
        loop(2, lambda i: outer(i + 2 * g))

    r1s, cbs = (r1a, r1b, r1c), (cba, cbb, cbc)
    s1s, r2s, s2s, r3s = (s1a, s1b, s1c), (r2a, r2b, r2c), (s2a, s2b, s2c), (r3a, r3b, r3c)
    lo, hi = pl.ds(0, 2), pl.ds(2, 2)
    for c in range(3):
        me = coord[c]
        send(blocks[c].at[(me + 2) % 4, lo], r1s[c].at[0], RA0 + 6 * c, at(c, 1))
        send(blocks[c].at[(me + 2) % 4, hi], r1s[c].at[1], RA0 + 6 * c + 1, at(c, -1))
    for c in range(3):
        me = coord[c]
        send(blocks[c].at[(me + 1) % 4, hi], r1s[c].at[2], RA0 + 6 * c + 2, at(c, 1))
        send(blocks[c].at[(me + 3) % 4, lo], r1s[c].at[3], RA0 + 6 * c + 3, at(c, -1))

    def back_send(pos, xx):
        blk = xx * 2 + q
        g = lax.dot_general(cotp[...], wg[xx], (((1,), (1,)), ((), ())), preferred_element_type=F32).astype(BF16)
        finp[pos] = g
        ga[blk] = finp[pos, rows(q, ROWS), :]
        send(finp.at[pos, rows(1 - q, ROWS)], ga.at[blk], GA0 + pos, partner)

    back_send(3, x)
    weights_end(left, 0)
    back_send(0, left)
    weights_end(right, 1)
    back_send(1, right)
    weights_end(far, 2)
    back_send(2, far)

    def join(c):
        me = coord[c]
        for h, idx, off in ((lo, 0, 1), (hi, 1, -1)):
            got(r1s[c].at[idx], RA0 + 6 * c + idx)
            own = blocks[c].at[(me + off) % 4, h]

            def add(i, own=own, idx=idx):
                a, b = i // 4, i % 4
                total = own[a, b].astype(F32) + r1s[c][idx, a, b].astype(F32)
                cbs[c][idx, a, b] = total.astype(BF16)

            loop(8, add)
            send(cbs[c].at[idx], r1s[c].at[4 + idx], RA0 + 6 * c + 4 + idx, at(c, off))

    for c in range(3):
        join(c)

    for pos, off in ((3, 0), (0, 3), (1, 1), (2, 2)):
        got(ga.at[((x + off) % 4) * 2 + 1 - q], GA0 + pos)

    sum2[...] = jnp.zeros((ROWS, 128), F32)
    halv = sum1
    halv[...] = jnp.zeros((ROWS, 128), F32)

    def grad_block(i):
        ln = lanes(i)
        gain = tkf[TAPS : TAPS + 1, ln]
        gsum = jnp.zeros((8, 128), F32)
        for jb in range(4):
            at_rows = pl.ds(64 * jb, 64)
            up = ga[i // 2, at_rows, lanes(i % 2)].astype(F32)
            gn = up * fwd[i, at_rows, :]
            ce = cen[i, at_rows, :]
            prod = gn * ce
            gsum = gsum + jnp.sum(prod.reshape(8, 8, 128), axis=0)
            gc = gn * gain
            fwd[i, at_rows, :] = gc
            sum1[at_rows, :] += gc
            sum2[at_rows, :] += prod * gain
        gkp[i, TAPS : TAPS + 1, :] = jnp.sum(gsum, axis=0, keepdims=True)

    loop(NSP, grad_block)
    m1 = jnp.sum(sum1[...], axis=1, keepdims=True) * (1.0 / D)
    m2 = jnp.sum(sum2[...], axis=1, keepdims=True) * (1.0 / D)
    sum1[...] = jnp.broadcast_to(m1, (ROWS, 128))
    sum2[...] = jnp.broadcast_to(m2, (ROWS, 128))

    def norm_block(i):
        ln = lanes(i)
        for jb in range(4):
            at_rows = pl.ds(64 * jb, 64)
            fwd[i, at_rows, :] = (
                fwd[i, at_rows, :] - sum1[at_rows, :] - cen[i, at_rows, :] * sum2[at_rows, :]
            ) * inv_b[at_rows, :]
        hal[:, ln] = fwd[i, pl.ds(0, SEG, stride=8), :]

    loop(NSP, norm_block)

    def margin_copy():
        return copy(hal, halr, GC0, {"sp": (s + NSP - 1) % NSP, "dp": d})

    @pl.when(s > 0)
    def _():
        margin_copy().start()

    def tap_block(i):
        col, kb = i // 4, i % 4
        ln = lanes(col)
        acc = [None] * 8
        window = {}
        for j in range(SEG):
            g = fwd[col, pl.ds(8 * j, 8), :]
            for o in range(8):
                if j - o not in window:
                    window[j - o] = ext[col, pl.ds(pl.multiple_of((SEG + j - o - kb * 8) * 8, 8), 8), :]
                term = g * window[j - o]
                acc[o] = term if acc[o] is None else acc[o] + term
        tops = [jnp.sum(a, axis=0, keepdims=True) for a in acc]
        for o in range(7):
            gkp[col, pl.ds(kb * 8 + o, 1), :] = tops[o]

        @pl.when(kb < 3)
        def _():
            gkp[col, pl.ds(kb * 8 + 7, 1), :] = tops[7]

    loop(64, tap_block)

    def send_gk(r):
        dst = (s + r + 1) % NSP
        copy(gkp.at[dst], gkr.at[r], GK0 + r, {"sp": dst, "dp": d}).start()

    loop(NSP - 1, send_gk)

    def stage1(c):
        got(r1s[c].at[2], RA0 + 6 * c + 2)
        got(r1s[c].at[3], RA0 + 6 * c + 3)
        got(r1s[c].at[4], RA0 + 6 * c + 4)
        got(r1s[c].at[5], RA0 + 6 * c + 5)
        me = coord[c]

        def add(i):
            a, b = i // 4, i % 4
            s1s[c][a, b] = (
                blocks[c][me, a, b].astype(F32) + r1s[c][4, a, b].astype(F32) + r1s[c][3, a, b].astype(F32)
            ).astype(BF16)
            s1s[c][a + 2, b] = (
                blocks[c][me, a + 2, b].astype(F32) + r1s[c][2, a, b].astype(F32) + r1s[c][5, a, b].astype(F32)
            ).astype(BF16)

        loop(8, add)
        axis = (c + 1) % 3
        for r in range(1, 4):
            send(s1s[c].at[(coord[axis] + r) % 4], r2s[c].at[r - 1], RB0 + 3 * c + r - 1, at(axis, r))

    def stage2(c):
        axis, last = (c + 1) % 3, (c + 2) % 3
        for r in range(1, 4):
            got(r2s[c].at[r - 1], RB0 + 3 * c + r - 1)

        def add(i):
            total = s1s[c][coord[axis], i].astype(F32)
            for r in range(3):
                total = total + r2s[c][r, i].astype(F32)
            s2s[c][i] = total.astype(BF16)

        loop(4, add)
        for r in range(1, 4):
            send(s2s[c].at[(coord[last] + r) % 4], r3s[c].at[r - 1], RC0 + 3 * c + r - 1, at(last, r))

    factor = float(NSP * NDP * ROWS) ** (-0.5)

    def stage3(c):
        last = (c + 2) % 3
        first, size = COLOURS[c]
        for r in range(1, 4):
            got(r3s[c].at[r - 1], RC0 + 3 * c + r - 1)
        mine = coord[last]
        for to_partner in (False, True):
            h = (1 - q) if to_partner else q
            part = rows(h, 16)
            total = s2s[c][mine, part, :].astype(F32)
            for r in range(3):
                total = total + r3s[c][r, part, :].astype(F32)
            total = total * factor
            if to_partner:
                fins[:, first : first + size] = total
            else:
                ow_ref[:, pl.ds(pl.multiple_of(q * HALF + first, 128), size)] = total

    for c in range(3):
        stage1(c)

    @pl.when(s < NSP - 1)
    def _():
        copy(halr, halr, GC0, partner).wait_recv()

    @pl.when(s == NSP - 1)
    def _():
        halr[...] = jnp.zeros((SEG, D), F32)

    def margin(i):
        ln = lanes(i)
        fwd[i, pl.ds(ROWS, 240), :] = fwd[i, pl.ds(1, 240), :]
        fwd[i, pl.ds(ROWS + 7, SEG, stride=8), :] = halr[:, ln]

    def back_block(i):
        col, jb = i // 4, i % 4
        ln = lanes(col)
        window = {o: fwd[col, pl.ds(pl.multiple_of((jb * 8 + o) * 8, 8), 8), :] for o in range(TAPS + 7)}
        acc = [None] * 8
        for k in range(TAPS):
            w = jnp.broadcast_to(tkf[k : k + 1, ln], (8, 128))
            for o in range(8):
                term = w * window[o + k]
                acc[o] = term if acc[o] is None else acc[o] + term
        for o in range(0, 8, 2):
            at_rows = pl.ds(pl.multiple_of((jb * 8 + o) * 8, 16), 16)
            ggp[at_rows, ln] = jnp.concatenate([acc[o], acc[o + 1]], axis=0).astype(BF16)

    out = []

    def finish(g):
        def body(i):
            cols = lanes(i + 2 * g, 256)
            grad = jnp.dot(permt[...], ggp[:, cols], preferred_element_type=F32)
            sg = sig[:, cols]
            gvo[:, cols] = (grad * sg).astype(BF16)
            ggo[:, cols] = (grad * val[:, cols].astype(F32) * sg * (1.0 - sg)).astype(BF16)

        loop(2, body)
        cols = pl.ds(512 * g, 512)
        for c in (
            pltpu.make_async_copy(gvo.at[:, cols], gv_hbm.at[:, cols], lsem.at[4 + 2 * g]),
            pltpu.make_async_copy(ggo.at[:, cols], gg_hbm.at[:, cols], lsem.at[5 + 2 * g]),
        ):
            c.start()
            out.append(c)

    def group(g):
        loop(4, lambda i: margin(i + 4 * g))
        loop(16, lambda i: back_block(i + 16 * g))
        finish(g)

    group(0)

    def got_gk(r):
        got(gkr.at[r], GK0 + r)

    loop(NSP - 1, got_gk)
    total = gkp[s]
    for r in range(NSP - 1):
        total = total + gkr[r]
    gdo[...] = total

    def send_gd(r):
        copy(gdo, gdr.at[r], GD0 + r, {"sp": s, "dp": (d + r + 1) % NDP}).start()

    loop(NDP - 1, send_gd)
    group(1)
    for c in range(3):
        stage2(c)
    group(2)
    for c in range(3):
        stage3(c)
    send(fins, finr, FIN0, partner)
    group(3)

    def got_gd(r):
        got(gdr.at[r], GD0 + r)

    loop(NDP - 1, got_gd)
    total = gdo[...]
    for r in range(NDP - 1):
        total = total + gdr[r]
    gk_ref[...] = total * factor
    got(finr, FIN0)
    ow_ref[:, lanes(1 - q, HALF)] = finr[...]

    for c in sent:
        c.wait_send()

    def drain_sp(r):
        copy(tkall.at[s], tkall.at[s], TAP0 + r, partner).wait_send()
        copy(gkp.at[s], gkr.at[r], GK0 + r, partner).wait_send()

    loop(NSP - 1, drain_sp)

    def drain_dp(r):
        copy(gdo, gdr.at[r], GD0 + r, partner).wait_send()

    loop(NDP - 1, drain_dp)

    @pl.when(s < NSP - 1)
    def _():
        halo_copy().wait_send()

    @pl.when(s > 0)
    def _():
        margin_copy().wait_send()

    for c in out:
        c.wait()


def shards(out_cotangent, value_pre, gate_pre, out_weight, conv_kernel, norm_gain):
    hbm = pl.BlockSpec(memory_space=pl.ANY)
    vmem = pl.BlockSpec(memory_space=pltpu.VMEM)
    sizes = [size for _, size in COLOURS]
    scratch = [
        ((2, ROWS, D), BF16),
        ((2 * ROWS, D), BF16),
        ((ROWS, D), BF16),
        ((ROWS, D), BF16),
        ((ROWS, D), F32),
        ((ROWS + 32, D), BF16),
        ((NSP, 2 * ROWS, 128), F32),
        ((NSP, ROWS, 128), F32),
        ((NSP, 2 * ROWS, 128), F32),
        ((2 * ROWS, D), BF16),
        ((4, ROWS, D), BF16),
        ((8, ROWS, ROWS), BF16),
        ((32, 128), F32),
        ((NSP, 32, 128), BF16),
        ((32, D), F32),
        ((ROWS, 128), F32),
        ((ROWS, 128), F32),
        ((ROWS, 128), F32),
        ((SEG, D), F32),
        ((SEG, D), F32),
        ((ROWS, D), BF16),
        ((ROWS, D), BF16),
        ((ROWS, D), BF16),
        ((NSP, 32, 128), F32),
        ((NSP - 1, 32, 128), F32),
        ((32, 128), F32),
        ((NDP - 1, 32, 128), F32),
    ]
    scratch += [((4, 4, 4, 32, f), BF16) for f in sizes]
    scratch += [((6, 2, 4, 32, f), BF16) for f in sizes]
    scratch += [((2, 2, 4, 32, f), BF16) for f in sizes]
    scratch += [((4, 4, 32, f), BF16) for f in sizes]
    scratch += [((3, 4, 32, f), BF16) for f in sizes]
    scratch += [((4, 32, f), BF16) for f in sizes]
    scratch += [((3, 32, f), BF16) for f in sizes]
    scratch += [
        ((4, 2 * ROWS, ROWS), BF16),
        ((16, HALF), F32),
        ((16, HALF), F32),
        ((ROWS, ROWS), BF16),
        ((ROWS, ROWS), BF16),
    ]
    grad_value, grad_gate, grad_weight, grad_taps = pl.pallas_call(
        kernel,
        out_shape=(
            jax.ShapeDtypeStruct((ROWS, D), BF16),
            jax.ShapeDtypeStruct((ROWS, D), BF16),
            jax.ShapeDtypeStruct((16, D), F32),
            jax.ShapeDtypeStruct((32, 128), F32),
        ),
        in_specs=[hbm, hbm, hbm, hbm, vmem, vmem],
        out_specs=(hbm, hbm, vmem, vmem),
        scratch_shapes=[pltpu.VMEM(shape, kind) for shape, kind in scratch]
        + [pltpu.SemaphoreType.DMA((NSEM,)), pltpu.SemaphoreType.DMA((NSEM,)), pltpu.SemaphoreType.DMA((12,))],
        compiler_params=pltpu.CompilerParams(
            collective_id=0, has_side_effects=True, vmem_limit_bytes=60 * 1024 * 1024
        ),
    )(out_cotangent[0], value_pre[0], gate_pre[0], out_weight, conv_kernel, norm_gain[None])
    return (grad_value[None], grad_gate[None], grad_weight, grad_taps[:TAPS], grad_taps[TAPS])


def solution(mesh):
    placed = (
        P("dp", "sp", None),
        P("dp", "sp", None),
        P("dp", "sp", None),
        P("dp", None),
        P(None, "sp"),
        P("sp"),
    )
    return jax.shard_map(
        shards,
        mesh=mesh,
        in_specs=placed,
        out_specs=(
            P("dp", "sp", None),
            P("dp", "sp", None),
            P(("sp", "dp"), None),
            P(None, "sp"),
            P("sp"),
        ),
        check_vma=False,
    )
```

```python
import functools

import jax
import jax.numpy as jnp
from jax import lax
from jax.experimental import pallas as pl
from jax.experimental.pallas import tpu as pltpu
from jax.sharding import PartitionSpec as P

EPS = 1e-05
F32 = jnp.float32
BF16 = jnp.bfloat16
MESH = pl.DeviceIdType.MESH

ROWS = 256
SEG = 16
D = 2048
HALF = 1024
TAPS = 31
NSP = 16
NDP = 8
WX_COLS, WY_COLS, WZ_COLS = (0, 512), (512, 768), (1280, 768)
COLOURS = ((0, 384), (384, 384), (768, 256))

TAP0 = 0
COT0 = TAP0 + 16
HALO0 = COT0 + 1
WX0 = HALO0 + 1
WY0 = WX0 + 12
WZ0 = WY0 + 12
ACT0 = WZ0 + 12
GA0 = ACT0 + 4
RA0 = GA0 + 4
RB0 = RA0 + 18
RC0 = RB0 + 9
GK0 = RC0 + 9
GD0 = GK0 + 16
GC0 = GD0 + 8
FIN0 = GC0 + 1
NSEM = FIN0 + 1


def sigmoid(x):
    return 0.5 * jnp.tanh(0.5 * x) + 0.5


def lanes(i, n=128):
    return pl.ds(pl.multiple_of(i * n, n), n)


def rows(i, n):
    return pl.ds(pl.multiple_of(i * n, n), n)


def loop(n, body):
    def step(i, c):
        body(i)
        return c

    lax.fori_loop(0, n, step, 0)


def kernel(
    cot_hbm,
    val_hbm,
    gate_hbm,
    w_hbm,
    taps_in,
    gain_in,
    gv_hbm,
    gg_hbm,
    ow_ref,
    gk_ref,
    cotraw,
    cotp,
    val,
    gate,
    sig,
    gext,
    ext,
    cen,
    fwd,
    act,
    wg,
    ga,
    tkown,
    tkall,
    taps,
    gains,
    sum1,
    sum2,
    inv_b,
    later,
    gcp,
    gcraw,
    ggp,
    gvo,
    ggo,
    gkp,
    gkr,
    gdo,
    gdr,
    pa,
    pb,
    pc,
    r1a,
    r1b,
    r1c,
    cba,
    cbb,
    cbc,
    s1a,
    s1b,
    s1c,
    r2a,
    r2b,
    r2c,
    s2a,
    s2b,
    s2c,
    r3a,
    r3b,
    r3c,
    finp,
    fins,
    finr,
    perm,
    ssem,
    rsem,
    lsem,
):
    s = lax.axis_index("sp")
    d = lax.axis_index("dp")
    z, y = s // 4, s % 4
    x, q = d // 2, d % 2

    def at(axis, off):
        if axis == 0:
            return {"sp": s, "dp": ((x + off) % 4) * 2 + q}
        if axis == 1:
            return {"sp": z * 4 + (y + off) % 4, "dp": d}
        return {"sp": ((z + off) % 4) * 4 + y, "dp": d}

    partner = {"sp": s, "dp": x * 2 + (1 - q)}
    coord = (x, y, z)

    sent = []

    def copy(src, dst, i, dev):
        return pltpu.make_async_remote_copy(
            src_ref=src, dst_ref=dst, send_sem=ssem.at[i], recv_sem=rsem.at[i], device_id=dev, device_id_type=MESH
        )

    def send(src, dst, i, dev):
        c = copy(src, dst, i, dev)
        c.start()
        sent.append(c)

    def got(dst, i):
        copy(dst, dst, i, partner).wait_recv()

    local = [
        pltpu.make_async_copy(w_hbm, wg.at[x], lsem.at[0]),
        pltpu.make_async_copy(val_hbm, val, lsem.at[1]),
        pltpu.make_async_copy(gate_hbm, gate, lsem.at[2]),
        pltpu.make_async_copy(cot_hbm, cotraw.at[q], lsem.at[3]),
    ]
    for c in local:
        c.start()
    barrier = pltpu.get_barrier_semaphore()

    def greet_sp(r):
        pl.semaphore_signal(barrier, inc=1, device_id={"sp": (s + r + 1) % NSP, "dp": d}, device_id_type=MESH)

    def greet_dp(r):
        pl.semaphore_signal(barrier, inc=1, device_id={"sp": s, "dp": (d + r + 1) % NDP}, device_id_type=MESH)

    loop(NSP - 1, greet_sp)
    loop(NDP - 1, greet_dp)
    tkown[0:TAPS, :] = taps_in[...].astype(F32)
    tkown[TAPS : TAPS + 1, :] = gain_in[...].astype(F32)
    tkall[s] = tkown[...].astype(BF16)
    r_io = lax.broadcasted_iota(jnp.int32, (ROWS, ROWS), 0)
    t_io = lax.broadcasted_iota(jnp.int32, (ROWS, ROWS), 1)
    perm[...] = jnp.where(t_io == (r_io & 15) * SEG + (r_io >> 4), 1.0, 0.0).astype(BF16)
    pl.semaphore_wait(barrier, NSP - 1 + NDP - 1)

    def piece(cols, size):
        def at_quarter(xx, quarter, h=None):
            n, first = (size, quarter * size) if h is None else (size // 2, quarter * size + h * (size // 2))
            return wg.at[xx, pl.ds(pl.multiple_of(first, n), n), pl.ds(*cols)]

        return at_quarter

    wx, wy, wz = piece(WX_COLS, ROWS), piece(WY_COLS, 64), piece(WZ_COLS, 64)

    local[0].wait()
    for i, off in ((0, 1), (1, -1)):
        send(wy(x, y), wy(x, y), WX0 + i, at(0, off))
    for i, off in ((0, 1), (1, -1)):
        send(wz(x, z), wz(x, z), WX0 + 2 + i, at(0, off))

    def send_taps(r):
        copy(tkall.at[s], tkall.at[s], TAP0 + r, {"sp": (s + r + 1) % NSP, "dp": d}).start()

    loop(NSP - 1, send_taps)

    local[1].wait()
    local[2].wait()

    def gate_block(i):
        at_rows = rows(ROWS // 32 - 1 - i, 32)
        sg = sigmoid(gate[at_rows, :].astype(F32))
        sig[at_rows, :] = sg
        gext[pl.ds(pl.multiple_of((ROWS // 32 - i) * 32, 32), 32), :] = (val[at_rows, :].astype(F32) * sg).astype(BF16)

    gate_block(0)

    def halo_copy():
        return copy(gext.at[pl.ds(ROWS, 32)], gext.at[pl.ds(0, 32)], HALO0, {"sp": (s + 1) % NSP, "dp": d})

    @pl.when(s < NSP - 1)
    def _():
        halo_copy().start()

    local[3].wait()
    send(cotraw.at[q], cotraw.at[q], COT0, partner)
    loop(ROWS // 32 - 1, lambda i: gate_block(i + 1))

    left, right, far = (x + 3) % 4, (x + 1) % 4, (x + 2) % 4
    both = ((0, 1), (1, -1))

    def along_x(part, quarter, base):
        for i, off in both:
            src = (x - off) % 4
            got(part(src, quarter), WX0 + base + i)
            send(part(src, quarter, i), part(src, quarter, i), WX0 + 6 + base + i, at(0, off))

    def far_along_x(part, quarter, base):
        for i, _ in both:
            got(part(far, quarter, i), WX0 + 6 + base + i)

    def across(axis, xx, pos):
        part, here, base = ((wy, y, WY0), (wz, z, WZ0))[axis - 1]
        for i, off in both:
            send(part(xx, here), part(xx, here), base + 4 * pos + i, at(axis, off))

    def across_on(axis, xx, pos):
        part, here, base = ((wy, y, WY0), (wz, z, WZ0))[axis - 1]
        for i, off in both:
            quarter = (here - off) % 4
            got(part(xx, quarter), base + 4 * pos + i)
            send(part(xx, quarter, i), part(xx, quarter, i), base + 4 * pos + 2 + i, at(axis, off))

    def across_end(axis, xx, pos):
        part, here, base = ((wy, y, WY0), (wz, z, WZ0))[axis - 1]
        for i, _ in both:
            got(part(xx, (here + 2) % 4, i), base + 4 * pos + 2 + i)

    def weights1():
        along_x(wy, y, 0)
        across(1, left, 0)
        across(1, right, 1)

    def weights2():
        along_x(wz, z, 2)
        across(2, left, 0)
        across(2, right, 1)
        for i, off in both:
            send(wx(x, 0), wx(x, 0), WX0 + 4 + i, at(0, off))

    def weights3():
        far_along_x(wy, y, 0)
        across(1, far, 2)
        across_on(1, left, 0)

    def weights4():
        far_along_x(wz, z, 2)
        across(2, far, 2)
        across_on(1, right, 1)
        across_on(2, left, 0)

    def weights5():
        across_on(2, right, 1)
        across_on(1, far, 2)
        along_x(wx, 0, 4)

    def weights6():
        across_on(2, far, 2)

    def weights_end(xx, pos):
        across_end(1, xx, pos)
        across_end(2, xx, pos)
        if pos == 2:
            far_along_x(wx, 0, 4)

    def spread(src, first, dst, base):
        def body(n):
            block = jnp.dot(perm[...], src[pl.ds(first, ROWS), lanes(n, 1024)], preferred_element_type=F32)
            block = block.astype(BF16)
            for i in range(8):
                dst[n * 8 + i, pl.ds(base, ROWS), :] = block[:, 128 * i : 128 * i + 128]

        loop(2, body)

    spread(gext, 32, ext, 2 * ROWS)

    def spread_cot(core):
        def body(n):
            block = jnp.dot(perm[...], cotraw[core, :, lanes(n, 1024)], preferred_element_type=F32)
            cotp[rows(core, ROWS), lanes(n, 1024)] = block.astype(BF16)

        loop(2, body)

    spread_cot(q)
    got(cotraw.at[1 - q], COT0)
    spread_cot(1 - q)

    @pl.when(s > 0)
    def _():
        got(gext.at[pl.ds(0, 32)], HALO0)

    @pl.when(s == 0)
    def _():
        gext[0:32, :] = jnp.zeros((32, D), BF16)

    weights1()
    spread(gext, 16, ext, ROWS)
    spread(gext, 0, ext, 0)

    def got_taps(r):
        src = (s + NSP - 1 - r) % NSP
        got(tkall.at[src], TAP0 + r)

    loop(NSP - 1, got_taps)

    def widen(i):
        t = tkall[i].astype(F32)
        gains[:, lanes(i)] = jnp.broadcast_to(t[TAPS : TAPS + 1], (16, 128))
        for k in range(TAPS):
            taps[i, 16 * k : 16 * k + 16, :] = jnp.broadcast_to(t[k : k + 1], (16, 128)).astype(BF16)

    loop(NSP, widen)

    def filtered(col, src, shift, emit):
        tiles, weights = src.at[col], taps.at[col]
        for j0 in range(0, SEG, 4):
            acc = [None] * 4
            for k in range(TAPS):
                for o in range(4):
                    at_row = 16 * shift(j0 + o, k)
                    term = weights[16 * k : 16 * k + 16, :].astype(F32) * tiles[at_row : at_row + 16, :].astype(F32)
                    acc[o] = term if acc[o] is None else acc[o] + term
            for o in range(4):
                emit(j0 + o, acc[o])

    def conv_block(col):
        dst = cen.at[col]

        def emit(j, v):
            dst[16 * j : 16 * j + 16, :] = v

        filtered(col, ext, lambda j, k: j - k + 2 * SEG, emit)

    loop(NSP, conv_block)

    weights2()

    def conv_sums(j):
        at_rows = rows(j, 16)
        one = two = None
        for col in range(NSP):
            v = cen[col, at_rows, :]
            one = v if one is None else one + v
            two = v * v if two is None else two + v * v
        sum1[at_rows, :] = one
        sum2[at_rows, :] = two

    loop(SEG, conv_sums)
    mean = jnp.sum(sum1[...], axis=1, keepdims=True) * (1.0 / D)
    var = jnp.sum(sum2[...], axis=1, keepdims=True) * (1.0 / D) - mean * mean
    sum1[...] = jnp.broadcast_to(mean, (ROWS, 128))
    inv_b[...] = jnp.broadcast_to(lax.rsqrt(var + EPS), (ROWS, 128))

    def act_block(g, j):
        at_rows = rows(j, 16)
        m, iv = sum1[at_rows, :], inv_b[at_rows, :]
        for col in range(4 * g, 4 * g + 4):
            ln = pl.ds(128 * col, 128)
            centred = (cen[col, at_rows, :] - m) * iv
            cen[col, at_rows, :] = centred
            normed = centred * gains[:, ln]
            sg = sigmoid(normed)
            act[pl.ds(pl.multiple_of(q * ROWS + j * 16, 16), 16), ln] = (normed * sg).astype(BF16)
            fwd[col, at_rows, :] = sg * (1.0 + normed * (1.0 - sg))

    for g in range(4):
        loop(SEG, lambda j: act_block(g, j))
        part = act.at[rows(q, ROWS), pl.ds(512 * g, 512)]
        send(part, part, ACT0 + g, partner)
        if g == 1:
            weights3()

    weights4()

    blocks = (pa, pb, pc)
    half = lanes(q, HALF)

    def outer(cb):
        p = lax.dot_general(
            act[:, lanes(cb, 256)], cotp[:, half], (((0,), (0,)), ((), ())), preferred_element_type=F32
        ).astype(BF16)
        zz, y0 = cb // 2, (cb % 2) * 2
        for i in range(8):
            yy, xx = y0 + i // 4, i % 4
            piece = p[32 * i : 32 * i + 32]
            pa[xx, yy, zz] = piece[:, 0:384]
            pb[yy, zz, xx] = piece[:, 384:768]
            pc[zz, xx, yy] = piece[:, 768:1024]

    for g in range(4):
        got(act.at[rows(1 - q, ROWS), pl.ds(512 * g, 512)], ACT0 + g)
        loop(2, lambda i: outer(i + 2 * g))
        if g == 1:
            weights5()

    r1s, cbs = (r1a, r1b, r1c), (cba, cbb, cbc)
    s1s, r2s, s2s, r3s = (s1a, s1b, s1c), (r2a, r2b, r2c), (s2a, s2b, s2c), (r3a, r3b, r3c)
    lo, hi = pl.ds(0, 2), pl.ds(2, 2)
    weights6()
    for c in range(3):
        me = coord[c]
        send(blocks[c].at[(me + 2) % 4, lo], r1s[c].at[0], RA0 + 6 * c, at(c, 1))
        send(blocks[c].at[(me + 2) % 4, hi], r1s[c].at[1], RA0 + 6 * c + 1, at(c, -1))
    for c in range(3):
        me = coord[c]
        send(blocks[c].at[(me + 1) % 4, hi], r1s[c].at[2], RA0 + 6 * c + 2, at(c, 1))
        send(blocks[c].at[(me + 3) % 4, lo], r1s[c].at[3], RA0 + 6 * c + 3, at(c, -1))

    def back_send(pos, xx):
        blk = xx * 2 + q
        g = lax.dot_general(cotp[...], wg[xx], (((1,), (1,)), ((), ())), preferred_element_type=F32).astype(BF16)
        finp[pos] = g
        ga[blk] = finp[pos, rows(q, ROWS), :]
        send(finp.at[pos, rows(1 - q, ROWS)], ga.at[blk], GA0 + pos, partner)

    back_send(3, x)
    weights_end(left, 0)
    back_send(0, left)
    weights_end(right, 1)
    back_send(1, right)
    weights_end(far, 2)
    back_send(2, far)

    def join(c):
        me = coord[c]
        for h, idx, off in ((lo, 0, 1), (hi, 1, -1)):
            got(r1s[c].at[idx], RA0 + 6 * c + idx)
            own = blocks[c].at[(me + off) % 4, h]

            def add(i, own=own, idx=idx):
                a, b = i // 4, i % 4
                total = own[a, b].astype(F32) + r1s[c][idx, a, b].astype(F32)
                cbs[c][idx, a, b] = total.astype(BF16)

            loop(8, add)
            send(cbs[c].at[idx], r1s[c].at[4 + idx], RA0 + 6 * c + 4 + idx, at(c, off))

    for c in range(3):
        join(c)

    for pos, off in ((3, 0), (0, 3), (1, 1), (2, 2)):
        got(ga.at[((x + off) % 4) * 2 + 1 - q], GA0 + pos)

    def grad_block(j, gsums):
        at_rows = rows(j, 16)
        one = two = None
        out_sums = []
        for col in range(NSP):
            ln = pl.ds(128 * col, 128)
            gn = ga[col // 2, at_rows, pl.ds(128 * (col % 2), 128)].astype(F32) * fwd[col, at_rows, :]
            prod = gn * cen[col, at_rows, :]
            out_sums.append(gsums[col] + prod[0:8] + prod[8:16])
            gain = gains[:, ln]
            gc = gn * gain
            fwd[col, at_rows, :] = gc
            prod = prod * gain
            one = gc if one is None else one + gc
            two = prod if two is None else two + prod
        sum1[at_rows, :] = one
        sum2[at_rows, :] = two
        return out_sums

    gsums = lax.fori_loop(0, SEG, grad_block, [jnp.zeros((8, 128), F32)] * NSP)
    for col in range(NSP):
        gkp[col, TAPS : TAPS + 1, :] = jnp.sum(gsums[col], axis=0, keepdims=True)
    m1 = jnp.sum(sum1[...], axis=1, keepdims=True) * (1.0 / D)
    m2 = jnp.sum(sum2[...], axis=1, keepdims=True) * (1.0 / D)
    sum1[...] = jnp.broadcast_to(m1, (ROWS, 128))
    sum2[...] = jnp.broadcast_to(m2, (ROWS, 128))

    def norm_block(j):
        at_rows = rows(j, 16)
        a, b, iv = sum1[at_rows, :], sum2[at_rows, :], inv_b[at_rows, :]
        for col in range(NSP):
            v = ((fwd[col, at_rows, :] - a - cen[col, at_rows, :] * b) * iv).astype(BF16)
            later[col, at_rows, :] = v
            gcp[at_rows, pl.ds(128 * col, 128)] = v

    loop(SEG, norm_block)

    def in_order(n):
        block = jnp.dot(perm[...], gcp[:, lanes(n, 1024)], preferred_element_type=F32)
        gcraw[0:ROWS, lanes(n, 1024)] = block.astype(BF16)

    loop(2, in_order)

    def margin_copy():
        return copy(
            gcraw.at[pl.ds(0, 32)], gcraw.at[pl.ds(ROWS, 32)], GC0, {"sp": (s + NSP - 1) % NSP, "dp": d}
        )

    @pl.when(s > 0)
    def _():
        margin_copy().start()

    def tap_block(col):
        grads, tiles, sums = later.at[col], ext.at[col], gkp.at[col]
        for k0 in range(0, TAPS, 4):
            taps_here = range(k0, min(k0 + 4, TAPS))
            acc = {}
            for j in range(SEG):
                for k in taps_here:
                    at_row = 16 * (j - k + 2 * SEG)
                    term = grads[16 * j : 16 * j + 16, :].astype(F32) * tiles[at_row : at_row + 16, :].astype(F32)
                    acc[k] = term if j == 0 else acc[k] + term
            for k in taps_here:
                sums[k : k + 1, :] = jnp.sum(acc[k][0:8] + acc[k][8:16], axis=0, keepdims=True)

    loop(NSP, tap_block)

    def send_gk(r):
        dst = (s + r + 1) % NSP
        copy(gkp.at[dst], gkr.at[r], GK0 + r, {"sp": dst, "dp": d}).start()

    loop(NSP - 1, send_gk)

    def stage1(c):
        got(r1s[c].at[2], RA0 + 6 * c + 2)
        got(r1s[c].at[3], RA0 + 6 * c + 3)
        got(r1s[c].at[4], RA0 + 6 * c + 4)
        got(r1s[c].at[5], RA0 + 6 * c + 5)
        me = coord[c]

        def add(i):
            a, b = i // 4, i % 4
            s1s[c][a, b] = (
                blocks[c][me, a, b].astype(F32) + r1s[c][4, a, b].astype(F32) + r1s[c][3, a, b].astype(F32)
            ).astype(BF16)
            s1s[c][a + 2, b] = (
                blocks[c][me, a + 2, b].astype(F32) + r1s[c][2, a, b].astype(F32) + r1s[c][5, a, b].astype(F32)
            ).astype(BF16)

        loop(8, add)
        axis = (c + 1) % 3
        for r in range(1, 4):
            send(s1s[c].at[(coord[axis] + r) % 4], r2s[c].at[r - 1], RB0 + 3 * c + r - 1, at(axis, r))

    def stage2(c):
        axis, last = (c + 1) % 3, (c + 2) % 3
        for r in range(1, 4):
            got(r2s[c].at[r - 1], RB0 + 3 * c + r - 1)

        def add(i):
            total = s1s[c][coord[axis], i].astype(F32)
            for r in range(3):
                total = total + r2s[c][r, i].astype(F32)
            s2s[c][i] = total.astype(BF16)

        loop(4, add)
        for r in range(1, 4):
            send(s2s[c].at[(coord[last] + r) % 4], r3s[c].at[r - 1], RC0 + 3 * c + r - 1, at(last, r))

    factor = float(NSP * NDP * ROWS) ** (-0.5)

    def stage3(c):
        last = (c + 2) % 3
        first, size = COLOURS[c]
        for r in range(1, 4):
            got(r3s[c].at[r - 1], RC0 + 3 * c + r - 1)
        mine = coord[last]
        for to_partner in (False, True):
            h = (1 - q) if to_partner else q
            part = rows(h, 16)
            total = s2s[c][mine, part, :].astype(F32)
            for r in range(3):
                total = total + r3s[c][r, part, :].astype(F32)
            total = total * factor
            if to_partner:
                fins[:, first : first + size] = total
            else:
                ow_ref[:, pl.ds(pl.multiple_of(q * HALF + first, 128), size)] = total

    for c in range(3):
        stage1(c)

    @pl.when(s < NSP - 1)
    def _():
        got(gcraw.at[pl.ds(ROWS, 32)], GC0)

    @pl.when(s == NSP - 1)
    def _():
        gcraw[ROWS : ROWS + 32, :] = jnp.zeros((32, D), BF16)

    spread(gcraw, 16, later, ROWS)
    spread(gcraw, 32, later, 2 * ROWS)

    def back_block(col):
        ln = lanes(col)

        def emit(j, v):
            ggp[16 * j : 16 * j + 16, ln] = v.astype(BF16)

        filtered(col, later, lambda j, k: j + k, emit)

    out = []

    def finish(g):
        cols = pl.ds(512 * g, 512)
        grad = jnp.dot(perm[...], ggp[:, cols], preferred_element_type=F32)
        sg = sig[:, cols]
        gvo[:, cols] = (grad * sg).astype(BF16)
        ggo[:, cols] = (grad * val[:, cols].astype(F32) * sg * (1.0 - sg)).astype(BF16)
        for c in (
            pltpu.make_async_copy(gvo.at[:, cols], gv_hbm.at[:, cols], lsem.at[4 + 2 * g]),
            pltpu.make_async_copy(ggo.at[:, cols], gg_hbm.at[:, cols], lsem.at[5 + 2 * g]),
        ):
            c.start()
            out.append(c)

    def group(g):
        loop(4, lambda i: back_block(i + 4 * g))
        finish(g)

    group(0)

    def got_gk(r):
        got(gkr.at[r], GK0 + r)

    loop(NSP - 1, got_gk)
    total = gkp[s]
    for r in range(NSP - 1):
        total = total + gkr[r]
    gdo[...] = total

    def send_gd(r):
        copy(gdo, gdr.at[r], GD0 + r, {"sp": s, "dp": (d + r + 1) % NDP}).start()

    loop(NDP - 1, send_gd)
    group(1)
    for c in range(3):
        stage2(c)
    group(2)
    for c in range(3):
        stage3(c)
    send(fins, finr, FIN0, partner)
    group(3)

    def got_gd(r):
        got(gdr.at[r], GD0 + r)

    loop(NDP - 1, got_gd)
    total = gdo[...]
    for r in range(NDP - 1):
        total = total + gdr[r]
    gk_ref[...] = total * factor
    got(finr, FIN0)
    ow_ref[:, lanes(1 - q, HALF)] = finr[...]

    for c in sent:
        c.wait_send()

    def drain_sp(r):
        copy(tkall.at[s], tkall.at[s], TAP0 + r, partner).wait_send()
        copy(gkp.at[s], gkr.at[r], GK0 + r, partner).wait_send()

    loop(NSP - 1, drain_sp)

    def drain_dp(r):
        copy(gdo, gdr.at[r], GD0 + r, partner).wait_send()

    loop(NDP - 1, drain_dp)

    @pl.when(s < NSP - 1)
    def _():
        halo_copy().wait_send()

    @pl.when(s > 0)
    def _():
        margin_copy().wait_send()

    for c in out:
        c.wait()


def place(gv_in, gg_in, ow_in, gk_in, gv_hbm, gg_hbm, ow_hbm, taps_hbm, gain_hbm, gv, gg, ow, gk, tp, gn, lsem, ssem):
    ins, outs = [], []
    for i in range(4):
        at_rows = pl.ds(64 * i, 64)
        ins.append(pltpu.make_async_copy(gv_in.at[at_rows], gv.at[at_rows], lsem.at[2 * i]))
        outs.append(pltpu.make_async_copy(gv.at[at_rows], gv_hbm.at[at_rows], ssem.at[2 * i]))
        ins.append(pltpu.make_async_copy(gg_in.at[at_rows], gg.at[at_rows], lsem.at[2 * i + 1]))
        outs.append(pltpu.make_async_copy(gg.at[at_rows], gg_hbm.at[at_rows], ssem.at[2 * i + 1]))
    ins.append(pltpu.make_async_copy(ow_in, ow, lsem.at[8]))
    outs.append(pltpu.make_async_copy(ow, ow_hbm, ssem.at[8]))
    small = pltpu.make_async_copy(gk_in, gk, lsem.at[9])
    small.start()
    for c in ins:
        c.start()
    for c, o in zip(ins, outs):
        c.wait()
        o.start()
    small.wait()
    tp[...] = gk[0:TAPS, :]
    gn[...] = gk[TAPS : TAPS + 1, :]
    outs.append(pltpu.make_async_copy(tp, taps_hbm, ssem.at[9]))
    outs.append(pltpu.make_async_copy(gn, gain_hbm, ssem.at[10]))
    outs[-2].start()
    outs[-1].start()
    for o in outs:
        o.wait()


def shards(out_cotangent, value_pre, gate_pre, out_weight, conv_kernel, norm_gain):
    hbm = pl.BlockSpec(memory_space=pl.ANY)
    vmem = pl.BlockSpec(memory_space=pltpu.VMEM)
    sizes = [size for _, size in COLOURS]
    scratch = [
        ((2, ROWS, D), BF16),
        ((2 * ROWS, D), BF16),
        ((ROWS, D), BF16),
        ((ROWS, D), BF16),
        ((ROWS, D), F32),
        ((ROWS + 32, D), BF16),
        ((NSP, 3 * ROWS, 128), BF16),
        ((NSP, ROWS, 128), F32),
        ((NSP, ROWS, 128), F32),
        ((2 * ROWS, D), BF16),
        ((4, ROWS, D), BF16),
        ((8, ROWS, ROWS), BF16),
        ((32, 128), F32),
        ((NSP, 32, 128), BF16),
        ((NSP, 16 * TAPS, 128), BF16),
        ((16, D), F32),
        ((ROWS, 128), F32),
        ((ROWS, 128), F32),
        ((ROWS, 128), F32),
        ((NSP, 3 * ROWS, 128), BF16),
        ((ROWS, D), BF16),
        ((ROWS + 32, D), BF16),
        ((ROWS, D), BF16),
        ((ROWS, D), BF16),
        ((ROWS, D), BF16),
        ((NSP, 32, 128), F32),
        ((NSP - 1, 32, 128), F32),
        ((32, 128), F32),
        ((NDP - 1, 32, 128), F32),
    ]
    scratch += [((4, 4, 4, 32, f), BF16) for f in sizes]
    scratch += [((6, 2, 4, 32, f), BF16) for f in sizes]
    scratch += [((2, 2, 4, 32, f), BF16) for f in sizes]
    scratch += [((4, 4, 32, f), BF16) for f in sizes]
    scratch += [((3, 4, 32, f), BF16) for f in sizes]
    scratch += [((4, 32, f), BF16) for f in sizes]
    scratch += [((3, 32, f), BF16) for f in sizes]
    scratch += [
        ((4, 2 * ROWS, ROWS), BF16),
        ((16, HALF), F32),
        ((16, HALF), F32),
        ((ROWS, ROWS), BF16),
    ]
    grad_value, grad_gate, grad_weight, grad_taps = pl.pallas_call(
        kernel,
        out_shape=(
            jax.ShapeDtypeStruct((ROWS, D), BF16),
            jax.ShapeDtypeStruct((ROWS, D), BF16),
            jax.ShapeDtypeStruct((16, D), F32),
            jax.ShapeDtypeStruct((32, 128), F32),
        ),
        in_specs=[hbm, hbm, hbm, hbm, vmem, vmem],
        out_specs=(hbm, hbm, vmem, vmem),
        scratch_shapes=[pltpu.VMEM(shape, kind) for shape, kind in scratch]
        + [pltpu.SemaphoreType.DMA((NSEM,)), pltpu.SemaphoreType.DMA((NSEM,)), pltpu.SemaphoreType.DMA((12,))],
        compiler_params=pltpu.CompilerParams(
            collective_id=0, has_side_effects=True, vmem_limit_bytes=60 * 1024 * 1024
        ),
    )(out_cotangent[0], value_pre[0], gate_pre[0], out_weight, conv_kernel, norm_gain[None])
    grad_value, grad_gate, grad_weight, grad_kernel, grad_gain = pl.pallas_call(
        place,
        out_shape=(
            jax.ShapeDtypeStruct((ROWS, D), BF16),
            jax.ShapeDtypeStruct((ROWS, D), BF16),
            jax.ShapeDtypeStruct((16, D), F32),
            jax.ShapeDtypeStruct((TAPS, 128), F32),
            jax.ShapeDtypeStruct((1, 128), F32),
        ),
        in_specs=[hbm] * 4,
        out_specs=(hbm,) * 5,
        scratch_shapes=[
            pltpu.VMEM((ROWS, D), BF16),
            pltpu.VMEM((ROWS, D), BF16),
            pltpu.VMEM((16, D), F32),
            pltpu.VMEM((32, 128), F32),
            pltpu.VMEM((TAPS, 128), F32),
            pltpu.VMEM((1, 128), F32),
            pltpu.SemaphoreType.DMA((10,)),
            pltpu.SemaphoreType.DMA((11,)),
        ],
    )(grad_value, grad_gate, grad_weight, grad_taps)
    return (grad_value[None], grad_gate[None], grad_weight, grad_kernel, grad_gain[0])


def solution(mesh):
    placed = (
        P("dp", "sp", None),
        P("dp", "sp", None),
        P("dp", "sp", None),
        P("dp", None),
        P(None, "sp"),
        P("sp"),
    )
    return jax.shard_map(
        shards,
        mesh=mesh,
        in_specs=placed,
        out_specs=(
            P("dp", "sp", None),
            P("dp", "sp", None),
            P(("sp", "dp"), None),
            P(None, "sp"),
            P("sp"),
        ),
        check_vma=False,
    )
```

```python
import functools

import jax
import jax.numpy as jnp
from jax import lax
from jax.experimental import pallas as pl
from jax.experimental.pallas import tpu as pltpu
from jax.sharding import PartitionSpec as P

EPS = 1e-05
F32 = jnp.float32
BF16 = jnp.bfloat16
MESH = pl.DeviceIdType.MESH

ROWS = 256
SEG = 16
D = 2048
HALF = 1024
TAPS = 31
NSP = 16
NDP = 8
WX_COLS, WY_COLS, WZ_COLS = (0, 384), (384, 896), (1280, 768)
COLOURS = ((0, 384), (384, 256), (640, 384))

TAP0 = 0
COT0 = TAP0 + 16
HALO0 = COT0 + 1
WX0 = HALO0 + 1
WY0 = WX0 + 12
WZ0 = WY0 + 12
ACT0 = WZ0 + 12
GA0 = ACT0 + 4
RA0 = GA0 + 4
RB0 = RA0 + 18
RC0 = RB0 + 9
GK0 = RC0 + 21
GD0 = GK0 + 16
GC0 = GD0 + 8
NSEM = GC0 + 1


def sigmoid(x):
    return 0.5 * jnp.tanh(0.5 * x) + 0.5


def lanes(i, n=128):
    return pl.ds(pl.multiple_of(i * n, n), n)


def rows(i, n):
    return pl.ds(pl.multiple_of(i * n, n), n)


def loop(n, body):
    def step(i, c):
        body(i)
        return c

    lax.fori_loop(0, n, step, 0)


def kernel(
    cot_hbm,
    val_hbm,
    gate_hbm,
    w_hbm,
    taps_hbm,
    gain_hbm,
    gv_hbm,
    gg_hbm,
    ow_ref,
    gk_ref,
    cotraw,
    cotp,
    val,
    gate,
    sig,
    gext,
    ext,
    cen,
    fwd,
    act,
    wg,
    ga,
    tkown,
    tkall,
    taps,
    gains,
    sum1,
    sum2,
    inv_b,
    later,
    gcp,
    gcraw,
    ggp,
    gvo,
    ggo,
    gkp,
    gkr,
    gdo,
    gdr,
    pa,
    pb,
    pc,
    r1a,
    r1b,
    r1c,
    cba,
    cbb,
    cbc,
    s1a,
    s1b,
    s1c,
    r2a,
    r2b,
    r2c,
    s2a,
    s2b,
    s2c,
    r3a,
    r3b,
    r3c,
    finp,
    perm,
    taps_in,
    gain_in,
    ssem,
    rsem,
    lsem,
):
    s = lax.axis_index("sp")
    d = lax.axis_index("dp")
    z, y = s // 4, s % 4
    x, q = d // 2, d % 2

    def at(axis, off, core=None):
        dp = d if core is None else x * 2 + core
        if axis == 0:
            return {"sp": s, "dp": ((x + off) % 4) * 2 + (q if core is None else core)}
        if axis == 1:
            return {"sp": z * 4 + (y + off) % 4, "dp": dp}
        return {"sp": ((z + off) % 4) * 4 + y, "dp": dp}

    def slot(axis, off):
        return (off - 1) % 4 if axis == 2 else (coord[axis] + off) % 4

    partner = {"sp": s, "dp": x * 2 + (1 - q)}
    coord = (x, y, z)

    sent = []

    def copy(src, dst, i, dev):
        return pltpu.make_async_remote_copy(
            src_ref=src, dst_ref=dst, send_sem=ssem.at[i], recv_sem=rsem.at[i], device_id=dev, device_id_type=MESH
        )

    def send(src, dst, i, dev):
        c = copy(src, dst, i, dev)
        c.start()
        sent.append(c)

    def got(dst, i):
        copy(dst, dst, i, partner).wait_recv()

    local = [
        pltpu.make_async_copy(w_hbm, wg.at[x], lsem.at[0]),
        pltpu.make_async_copy(val_hbm, val, lsem.at[1]),
        pltpu.make_async_copy(gate_hbm, gate, lsem.at[2]),
        pltpu.make_async_copy(cot_hbm, cotraw.at[q], lsem.at[3]),
    ]
    small = [
        pltpu.make_async_copy(taps_hbm, taps_in, lsem.at[12]),
        pltpu.make_async_copy(gain_hbm, gain_in, lsem.at[13]),
    ]
    for c in (local[0], *small, *local[1:]):
        c.start()
    barrier = pltpu.get_barrier_semaphore()

    def greet_sp(r):
        pl.semaphore_signal(barrier, inc=1, device_id={"sp": (s + r + 1) % NSP, "dp": d}, device_id_type=MESH)

    def greet_dp(r):
        pl.semaphore_signal(barrier, inc=1, device_id={"sp": s, "dp": (d + r + 1) % NDP}, device_id_type=MESH)

    loop(NSP - 1, greet_sp)
    loop(NDP - 1, greet_dp)
    for axis in (1, 2):
        for r in (1, 2, 3):
            pl.semaphore_signal(barrier, inc=1, device_id=at(axis, r, 1 - q), device_id_type=MESH)
    r_io = lax.broadcasted_iota(jnp.int32, (ROWS, ROWS), 0)
    t_io = lax.broadcasted_iota(jnp.int32, (ROWS, ROWS), 1)
    perm[...] = jnp.where(t_io == (r_io & 15) * SEG + (r_io >> 4), 1.0, 0.0).astype(BF16)
    pl.semaphore_wait(barrier, NSP - 1 + NDP - 1 + 6)

    def piece(cols, size):
        def at_quarter(xx, quarter, h=None):
            n, first = (size, quarter * size) if h is None else (size // 2, quarter * size + h * (size // 2))
            return wg.at[xx, pl.ds(pl.multiple_of(first, n), n), pl.ds(*cols)]

        return at_quarter

    wx, wy, wz = piece(WX_COLS, ROWS), piece(WY_COLS, 64), piece(WZ_COLS, 64)

    local[0].wait()
    for i, off in ((0, 1), (1, -1)):
        send(wy(x, y), wy(x, y), WX0 + i, at(0, off))
    for i, off in ((0, 1), (1, -1)):
        send(wz(x, z), wz(x, z), WX0 + 2 + i, at(0, off))

    for c in small:
        c.wait()
    tkown[0:TAPS, :] = taps_in[...].astype(F32)
    tkown[TAPS : TAPS + 1, :] = gain_in[...].astype(F32)
    tkall[s] = tkown[...].astype(BF16)

    def send_taps(r):
        copy(tkall.at[s], tkall.at[s], TAP0 + r, {"sp": (s + r + 1) % NSP, "dp": d}).start()

    loop(NSP - 1, send_taps)

    local[1].wait()
    local[2].wait()

    def gate_block(i):
        at_rows = rows(ROWS // 32 - 1 - i, 32)
        sg = sigmoid(gate[at_rows, :].astype(F32))
        sig[at_rows, :] = sg
        gext[pl.ds(pl.multiple_of((ROWS // 32 - i) * 32, 32), 32), :] = (val[at_rows, :].astype(F32) * sg).astype(BF16)

    gate_block(0)

    def halo_copy():
        return copy(gext.at[pl.ds(ROWS, 32)], gext.at[pl.ds(0, 32)], HALO0, {"sp": (s + 1) % NSP, "dp": d})

    @pl.when(s < NSP - 1)
    def _():
        halo_copy().start()

    local[3].wait()
    send(cotraw.at[q], cotraw.at[q], COT0, partner)
    loop(ROWS // 32 - 1, lambda i: gate_block(i + 1))

    left, right, far = (x + 3) % 4, (x + 1) % 4, (x + 2) % 4
    both = ((0, 1), (1, -1))

    def along_x(part, quarter, base):
        for i, off in both:
            src = (x - off) % 4
            got(part(src, quarter), WX0 + base + i)
            send(part(src, quarter, i), part(src, quarter, i), WX0 + 6 + base + i, at(0, off))

    def far_along_x(part, quarter, base):
        for i, _ in both:
            got(part(far, quarter, i), WX0 + 6 + base + i)

    def across(axis, xx, pos):
        part, here, base = ((wy, y, WY0), (wz, z, WZ0))[axis - 1]
        for i, off in both:
            send(part(xx, here), part(xx, here), base + 4 * pos + i, at(axis, off))

    def across_on(axis, xx, pos):
        part, here, base = ((wy, y, WY0), (wz, z, WZ0))[axis - 1]
        for i, off in both:
            quarter = (here - off) % 4
            got(part(xx, quarter), base + 4 * pos + i)
            send(part(xx, quarter, i), part(xx, quarter, i), base + 4 * pos + 2 + i, at(axis, off))

    def across_end(axis, xx, pos):
        part, here, base = ((wy, y, WY0), (wz, z, WZ0))[axis - 1]
        for i, _ in both:
            got(part(xx, (here + 2) % 4, i), base + 4 * pos + 2 + i)

    def weights_end(xx, pos):
        across_end(1, xx, pos)
        across_end(2, xx, pos)
        if pos == 2:
            far_along_x(wx, 0, 4)

    def spread(src, first, dst, base):
        def body(n):
            block = jnp.dot(perm[...], src[pl.ds(first, ROWS), lanes(n, 1024)], preferred_element_type=F32)
            block = block.astype(BF16)
            for i in range(8):
                dst[n * 8 + i, pl.ds(base, ROWS), :] = block[:, 128 * i : 128 * i + 128]

        loop(2, body)

    spread(gext, 32, ext, 2 * ROWS)

    def spread_cot(core):
        def body(n):
            block = jnp.dot(perm[...], cotraw[core, :, lanes(n, 1024)], preferred_element_type=F32)
            cotp[rows(core, ROWS), lanes(n, 1024)] = block.astype(BF16)

        loop(2, body)

    spread_cot(q)
    got(cotraw.at[1 - q], COT0)
    spread_cot(1 - q)

    @pl.when(s > 0)
    def _():
        got(gext.at[pl.ds(0, 32)], HALO0)

    @pl.when(s == 0)
    def _():
        gext[0:32, :] = jnp.zeros((32, D), BF16)

    along_x(wy, y, 0)
    across(1, left, 0)
    across(1, right, 1)
    spread(gext, 16, ext, ROWS)
    spread(gext, 0, ext, 0)

    def got_taps(r):
        src = (s + NSP - 1 - r) % NSP
        got(tkall.at[src], TAP0 + r)

    loop(NSP - 1, got_taps)

    def widen(i):
        t = tkall[i].astype(F32)
        gains[:, lanes(i)] = jnp.broadcast_to(t[TAPS : TAPS + 1], (16, 128))
        for k in range(TAPS):
            taps[i, 16 * k : 16 * k + 16, :] = jnp.broadcast_to(t[k : k + 1], (16, 128)).astype(BF16)

    loop(NSP, widen)

    def filtered(col, src, shift, emit):
        tiles, weights = src.at[col], taps.at[col]
        for j0 in range(0, SEG, 4):
            acc = [None] * 4
            for k in range(TAPS):
                for o in range(4):
                    at_row = 16 * shift(j0 + o, k)
                    term = weights[16 * k : 16 * k + 16, :].astype(F32) * tiles[at_row : at_row + 16, :].astype(F32)
                    acc[o] = term if acc[o] is None else acc[o] + term
            for o in range(4):
                emit(j0 + o, acc[o])

    def conv_block(col):
        dst = cen.at[col]

        def emit(j, v):
            dst[16 * j : 16 * j + 16, :] = v

        filtered(col, ext, lambda j, k: j - k + 2 * SEG, emit)

    along_x(wz, z, 2)
    across(2, left, 0)
    across(2, right, 1)
    for i, off in both:
        send(wx(x, 0), wx(x, 0), WX0 + 4 + i, at(0, off))
    loop(NSP, conv_block)

    far_along_x(wy, y, 0)
    across(1, far, 2)

    def conv_sums(j):
        at_rows = rows(j, 16)
        one = two = None
        for col in range(NSP):
            v = cen[col, at_rows, :]
            one = v if one is None else one + v
            two = v * v if two is None else two + v * v
        sum1[at_rows, :] = one
        sum2[at_rows, :] = two

    loop(SEG, conv_sums)
    mean = jnp.sum(sum1[...], axis=1, keepdims=True) * (1.0 / D)
    var = jnp.sum(sum2[...], axis=1, keepdims=True) * (1.0 / D) - mean * mean
    sum1[...] = jnp.broadcast_to(mean, (ROWS, 128))
    inv_b[...] = jnp.broadcast_to(lax.rsqrt(var + EPS), (ROWS, 128))

    def act_block(g, j):
        at_rows = rows(j, 16)
        m, iv = sum1[at_rows, :], inv_b[at_rows, :]
        for i in range(4):
            col = 4 * g + i
            ln = lanes(col)
            centred = (cen[col, at_rows, :] - m) * iv
            cen[col, at_rows, :] = centred
            normed = centred * gains[:, ln]
            sg = sigmoid(normed)
            act[pl.ds(pl.multiple_of(q * ROWS + j * 16, 16), 16), ln] = (normed * sg).astype(BF16)
            fwd[col, at_rows, :] = sg * (1.0 + normed * (1.0 - sg))

    order = (1, 0, 2, 3)
    groups = [(z + 1 + zr) % 4 for zr in order]
    for pos, g in enumerate(groups):
        loop(SEG, lambda j, g=g: act_block(g, j))
        part = act.at[rows(q, ROWS), lanes(g, 512)]
        send(part, part, ACT0 + pos, partner)
        if pos == 1:
            across_on(1, left, 0)
        if pos == 3:
            far_along_x(wz, z, 2)
            across(2, far, 2)

    blocks = (pa, pb, pc)
    half = lanes(q, HALF)

    def outer(g, zr, i):
        p = lax.dot_general(
            act[:, lanes(2 * g + i, 256)], cotp[:, half], (((0,), (0,)), ((), ())), preferred_element_type=F32
        ).astype(BF16)
        for n in range(8):
            yy, xx = i * 2 + n // 4, n % 4
            part = p[32 * n : 32 * n + 32]
            pa[xx, yy, zr] = part[:, 0:384]
            pb[yy, zr, xx] = part[:, 384:640]
            pc[zr, xx, yy] = part[:, 640:1024]

    r1s, cbs = (r1a, r1b, r1c), (cba, cbb, cbc)
    s1s, r2s, s2s, r3s = (s1a, s1b, s1c), (r2a, r2b, r2c), (s2a, s2b, s2c), (r3a, r3b, r3c)
    firsts, lasts = pl.ds(0, 2), pl.ds(2, 2)

    def half_of(c, off, h):
        cut = (firsts, lasts)[h]
        if c == 0:
            return blocks[0].at[slot(0, off), :, cut]
        return blocks[c].at[slot(c, off), cut]

    def sums_far(c, h):
        send(half_of(c, 2, h), r1s[c].at[h], RA0 + 6 * c + h, at(c, (1, -1)[h]))

    def sums_alone(c, h):
        send(half_of(c, (-1, 1)[h], h), r1s[c].at[3 - h], RA0 + 6 * c + 3 - h, at(c, (-1, 1)[h]))

    for pos, (g, zr) in enumerate(zip(groups, order)):
        got(act.at[rows(1 - q, ROWS), lanes(g, 512)], ACT0 + pos)
        loop(2, lambda i, g=g, zr=zr: outer(g, zr, i))
        if pos == 0:
            across_on(2, left, 0)
            sums_far(2, 0)
            sums_far(2, 1)
        if pos == 1:
            across_on(1, right, 1)
            for c in (0, 1):
                sums_far(c, 0)
                sums_alone(c, 0)
        if pos == 2:
            across_on(2, right, 1)
        if pos == 3:
            across_on(1, far, 2)
            across_on(2, far, 2)
            along_x(wx, 0, 4)
            for c in (0, 1):
                sums_far(c, 1)
            for c in (0, 1):
                sums_alone(c, 1)
            sums_alone(2, 0)
            sums_alone(2, 1)

    def each(c, body):
        loop(8, (lambda i: body(i // 2, i % 2)) if c == 0 else (lambda i: body(i // 4, i % 4)))

    def join(c, h):
        got(r1s[c].at[h], RA0 + 6 * c + h)
        own = half_of(c, (1, -1)[h], h)

        def add(a, b):
            cbs[c][h, a, b] = (own[a, b].astype(F32) + r1s[c][h, a, b].astype(F32)).astype(BF16)

        each(c, add)
        send(cbs[c].at[h], r1s[c].at[4 + h], RA0 + 6 * c + 4 + h, at(c, (1, -1)[h]))

    def back_send(pos, xx):
        blk = xx * 2 + q
        g = lax.dot_general(cotp[...], wg[xx], (((1,), (1,)), ((), ())), preferred_element_type=F32).astype(BF16)
        finp[pos] = g
        ga[blk] = finp[pos, rows(q, ROWS), :]
        send(finp.at[pos, rows(1 - q, ROWS)], ga.at[blk], GA0 + pos, partner)

    back_send(3, x)
    weights_end(left, 0)
    back_send(0, left)
    weights_end(right, 1)
    back_send(1, right)
    join(2, 0)
    join(2, 1)
    weights_end(far, 2)
    back_send(2, far)

    for c in (1, 0):
        join(c, 0)
        join(c, 1)

    for pos, off in ((3, 0), (0, 3), (1, 1), (2, 2)):
        got(ga.at[((x + off) % 4) * 2 + 1 - q], GA0 + pos)

    def grad_block(j, gsums):
        at_rows = rows(j, 16)
        one = two = None
        out_sums = []
        for col in range(NSP):
            ln = pl.ds(128 * col, 128)
            gn = ga[col // 2, at_rows, pl.ds(128 * (col % 2), 128)].astype(F32) * fwd[col, at_rows, :]
            prod = gn * cen[col, at_rows, :]
            out_sums.append(gsums[col] + prod[0:8] + prod[8:16])
            gain = gains[:, ln]
            gc = gn * gain
            fwd[col, at_rows, :] = gc
            prod = prod * gain
            one = gc if one is None else one + gc
            two = prod if two is None else two + prod
        sum1[at_rows, :] = one
        sum2[at_rows, :] = two
        return out_sums

    gsums = lax.fori_loop(0, SEG, grad_block, [jnp.zeros((8, 128), F32)] * NSP)
    for col in range(NSP):
        gkp[col, TAPS : TAPS + 1, :] = jnp.sum(gsums[col], axis=0, keepdims=True)
    m1 = jnp.sum(sum1[...], axis=1, keepdims=True) * (1.0 / D)
    m2 = jnp.sum(sum2[...], axis=1, keepdims=True) * (1.0 / D)
    sum1[...] = jnp.broadcast_to(m1, (ROWS, 128))
    sum2[...] = jnp.broadcast_to(m2, (ROWS, 128))

    def norm_block(j):
        at_rows = rows(j, 16)
        a, b, iv = sum1[at_rows, :], sum2[at_rows, :], inv_b[at_rows, :]
        for col in range(NSP):
            v = ((fwd[col, at_rows, :] - a - cen[col, at_rows, :] * b) * iv).astype(BF16)
            later[col, at_rows, :] = v
            gcp[at_rows, pl.ds(128 * col, 128)] = v

    loop(SEG, norm_block)

    def in_order(n):
        block = jnp.dot(perm[...], gcp[:, lanes(n, 1024)], preferred_element_type=F32)
        gcraw[0:ROWS, lanes(n, 1024)] = block.astype(BF16)

    loop(2, in_order)

    def margin_copy():
        return copy(
            gcraw.at[pl.ds(0, 32)], gcraw.at[pl.ds(ROWS, 32)], GC0, {"sp": (s + NSP - 1) % NSP, "dp": d}
        )

    @pl.when(s > 0)
    def _():
        margin_copy().start()

    def tap_block(col):
        grads, tiles, sums = later.at[col], ext.at[col], gkp.at[col]
        for k0 in range(0, TAPS, 4):
            taps_here = range(k0, min(k0 + 4, TAPS))
            acc = {}
            for j in range(SEG):
                for k in taps_here:
                    at_row = 16 * (j - k + 2 * SEG)
                    term = grads[16 * j : 16 * j + 16, :].astype(F32) * tiles[at_row : at_row + 16, :].astype(F32)
                    acc[k] = term if j == 0 else acc[k] + term
            for k in taps_here:
                sums[k : k + 1, :] = jnp.sum(acc[k][0:8] + acc[k][8:16], axis=0, keepdims=True)

    loop(NSP, tap_block)

    def send_gk(r):
        dst = (s + r + 1) % NSP
        copy(gkp.at[dst], gkr.at[r], GK0 + r, {"sp": dst, "dp": d}).start()

    loop(NSP - 1, send_gk)

    def stage1(c):
        for n in range(2, 6):
            got(r1s[c].at[n], RA0 + 6 * c + n)
        for h, pair in ((0, (4, 3)), (1, (2, 5))):
            own = half_of(c, 0, h)
            dst = s1s[c].at[:, (firsts, lasts)[h]] if c == 0 else s1s[c].at[(firsts, lasts)[h]]

            def add(a, b, own=own, dst=dst, pair=pair):
                dst[a, b] = (
                    own[a, b].astype(F32) + r1s[c][pair[0], a, b].astype(F32) + r1s[c][pair[1], a, b].astype(F32)
                ).astype(BF16)

            each(c, add)
        axis = (c + 1) % 3
        for r in range(1, 4):
            send(s1s[c].at[slot(axis, r)], r2s[c].at[r - 1], RB0 + 3 * c + r - 1, at(axis, r))

    def stage2(c):
        axis, last = (c + 1) % 3, (c + 2) % 3
        for r in range(1, 4):
            got(r2s[c].at[r - 1], RB0 + 3 * c + r - 1)

        def add(i):
            total = s1s[c][slot(axis, 0), i].astype(F32)
            for r in range(3):
                total = total + r2s[c][r, i].astype(F32)
            s2s[c][i] = total.astype(BF16)

        loop(4, add)
        for r in range(1, 4):
            for other in range(2):
                core = 1 - q if other else q
                send(
                    s2s[c].at[slot(last, r), rows(core, 16)],
                    r3s[c].at[other, r],
                    RC0 + 7 * c + 2 * r + other - 1,
                    at(last, r, core),
                )
        send(s2s[c].at[slot(last, 0), rows(1 - q, 16)], r3s[c].at[1, 0], RC0 + 7 * c, partner)

    factor = float(NSP * NDP * ROWS) ** (-0.5)

    def stage3(c):
        last = (c + 2) % 3
        first, size = COLOURS[c]
        got(r3s[c].at[1, 0], RC0 + 7 * c)
        for r in range(1, 4):
            for other in range(2):
                got(r3s[c].at[other, r], RC0 + 7 * c + 2 * r + other - 1)
        for other in range(2):
            if other:
                total = r3s[c][1, 0].astype(F32)
            else:
                total = s2s[c][slot(last, 0), rows(q, 16), :].astype(F32)
            for r in range(1, 4):
                total = total + r3s[c][other, r].astype(F32)
            core = 1 - q if other else q
            ow_ref[:, pl.ds(pl.multiple_of(core * HALF + first, 128), size)] = total * factor

    for c in (2, 1, 0):
        stage1(c)

    @pl.when(s < NSP - 1)
    def _():
        got(gcraw.at[pl.ds(ROWS, 32)], GC0)

    @pl.when(s == NSP - 1)
    def _():
        gcraw[ROWS : ROWS + 32, :] = jnp.zeros((32, D), BF16)

    spread(gcraw, 16, later, ROWS)
    spread(gcraw, 32, later, 2 * ROWS)

    def back_block(col):
        ln = lanes(col)

        def emit(j, v):
            ggp[16 * j : 16 * j + 16, ln] = v.astype(BF16)

        filtered(col, later, lambda j, k: j + k, emit)

    out = []

    def finish(g):
        cols = pl.ds(512 * g, 512)
        grad = jnp.dot(perm[...], ggp[:, cols], preferred_element_type=F32)
        sg = sig[:, cols]
        gvo[:, cols] = (grad * sg).astype(BF16)
        ggo[:, cols] = (grad * val[:, cols].astype(F32) * sg * (1.0 - sg)).astype(BF16)
        for c in (
            pltpu.make_async_copy(gvo.at[:, cols], gv_hbm.at[:, cols], lsem.at[4 + 2 * g]),
            pltpu.make_async_copy(ggo.at[:, cols], gg_hbm.at[:, cols], lsem.at[5 + 2 * g]),
        ):
            c.start()
            out.append(c)

    def group(g):
        loop(4, lambda i: back_block(i + 4 * g))
        finish(g)

    group(0)

    def got_gk(r):
        got(gkr.at[r], GK0 + r)

    loop(NSP - 1, got_gk)
    total = gkp[s]
    for r in range(NSP - 1):
        total = total + gkr[r]
    gdo[...] = total

    def send_gd(r):
        copy(gdo, gdr.at[r], GD0 + r, {"sp": s, "dp": (d + r + 1) % NDP}).start()

    loop(NDP - 1, send_gd)
    group(1)
    for c in (2, 1, 0):
        stage2(c)
    group(2)
    group(3)
    for c in (2, 1, 0):
        stage3(c)

    def got_gd(r):
        got(gdr.at[r], GD0 + r)

    loop(NDP - 1, got_gd)
    total = gdo[...]
    for r in range(NDP - 1):
        total = total + gdr[r]
    gk_ref[...] = total * factor

    for c in sent:
        c.wait_send()

    def drain_sp(r):
        copy(tkall.at[s], tkall.at[s], TAP0 + r, partner).wait_send()
        copy(gkp.at[s], gkr.at[r], GK0 + r, partner).wait_send()

    loop(NSP - 1, drain_sp)

    def drain_dp(r):
        copy(gdo, gdr.at[r], GD0 + r, partner).wait_send()

    loop(NDP - 1, drain_dp)

    @pl.when(s < NSP - 1)
    def _():
        halo_copy().wait_send()

    @pl.when(s > 0)
    def _():
        margin_copy().wait_send()

    for c in out:
        c.wait()


def place(gv_in, gg_in, ow_in, gk_in, gv_hbm, gg_hbm, ow_hbm, taps_hbm, gain_hbm, gv, gg, ow, gk, tp, gn, lsem, ssem):
    ins, outs = [], []
    for i in range(4):
        at_rows = pl.ds(64 * i, 64)
        ins.append(pltpu.make_async_copy(gv_in.at[at_rows], gv.at[at_rows], lsem.at[2 * i]))
        outs.append(pltpu.make_async_copy(gv.at[at_rows], gv_hbm.at[at_rows], ssem.at[2 * i]))
        ins.append(pltpu.make_async_copy(gg_in.at[at_rows], gg.at[at_rows], lsem.at[2 * i + 1]))
        outs.append(pltpu.make_async_copy(gg.at[at_rows], gg_hbm.at[at_rows], ssem.at[2 * i + 1]))
    ins.append(pltpu.make_async_copy(ow_in, ow, lsem.at[8]))
    outs.append(pltpu.make_async_copy(ow, ow_hbm, ssem.at[8]))
    small = pltpu.make_async_copy(gk_in, gk, lsem.at[9])
    small.start()
    for c in ins:
        c.start()
    for c, o in zip(ins, outs):
        c.wait()
        o.start()
    small.wait()
    tp[...] = gk[0:TAPS, :]
    gn[...] = gk[TAPS : TAPS + 1, :]
    outs.append(pltpu.make_async_copy(tp, taps_hbm, ssem.at[9]))
    outs.append(pltpu.make_async_copy(gn, gain_hbm, ssem.at[10]))
    outs[-2].start()
    outs[-1].start()
    for o in outs:
        o.wait()


def shards(out_cotangent, value_pre, gate_pre, out_weight, conv_kernel, norm_gain):
    hbm = pl.BlockSpec(memory_space=pl.ANY)
    vmem = pl.BlockSpec(memory_space=pltpu.VMEM)
    sizes = [size for _, size in COLOURS]
    scratch = [
        ((2, ROWS, D), BF16),
        ((2 * ROWS, D), BF16),
        ((ROWS, D), BF16),
        ((ROWS, D), BF16),
        ((ROWS, D), F32),
        ((ROWS + 32, D), BF16),
        ((NSP, 3 * ROWS, 128), BF16),
        ((NSP, ROWS, 128), F32),
        ((NSP, ROWS, 128), F32),
        ((2 * ROWS, D), BF16),
        ((4, ROWS, D), BF16),
        ((8, ROWS, ROWS), BF16),
        ((32, 128), F32),
        ((NSP, 32, 128), BF16),
        ((NSP, 16 * TAPS, 128), BF16),
        ((16, D), F32),
        ((ROWS, 128), F32),
        ((ROWS, 128), F32),
        ((ROWS, 128), F32),
        ((NSP, 3 * ROWS, 128), BF16),
        ((ROWS, D), BF16),
        ((ROWS + 32, D), BF16),
        ((ROWS, D), BF16),
        ((ROWS, D), BF16),
        ((ROWS, D), BF16),
        ((NSP, 32, 128), F32),
        ((NSP - 1, 32, 128), F32),
        ((32, 128), F32),
        ((NDP - 1, 32, 128), F32),
    ]
    scratch += [((4, 4, 4, 32, f), BF16) for f in sizes]
    halves = [(4, 2), (2, 4), (2, 4)]
    scratch += [((6, *h, 32, f), BF16) for h, f in zip(halves, sizes)]
    scratch += [((2, *h, 32, f), BF16) for h, f in zip(halves, sizes)]
    scratch += [((4, 4, 32, f), BF16) for f in sizes]
    scratch += [((3, 4, 32, f), BF16) for f in sizes]
    scratch += [((4, 32, f), BF16) for f in sizes]
    scratch += [((2, 4, 16, f), BF16) for f in sizes]
    scratch += [
        ((4, 2 * ROWS, ROWS), BF16),
        ((ROWS, ROWS), BF16),
        ((TAPS, 128), BF16),
        ((1, 128), BF16),
    ]
    grad_value, grad_gate, grad_weight, grad_taps = pl.pallas_call(
        kernel,
        out_shape=(
            jax.ShapeDtypeStruct((ROWS, D), BF16),
            jax.ShapeDtypeStruct((ROWS, D), BF16),
            jax.ShapeDtypeStruct((16, D), F32),
            jax.ShapeDtypeStruct((32, 128), F32),
        ),
        in_specs=[pl.BlockSpec(memory_space=pltpu.HBM)] * 6,
        out_specs=(hbm, hbm, vmem, vmem),
        scratch_shapes=[pltpu.VMEM(shape, kind) for shape, kind in scratch]
        + [pltpu.SemaphoreType.DMA((NSEM,)), pltpu.SemaphoreType.DMA((NSEM,)), pltpu.SemaphoreType.DMA((14,))],
        compiler_params=pltpu.CompilerParams(
            collective_id=0, has_side_effects=True, vmem_limit_bytes=60 * 1024 * 1024
        ),
    )(out_cotangent[0], value_pre[0], gate_pre[0], out_weight, conv_kernel, norm_gain[None])
    grad_value, grad_gate, grad_weight, grad_kernel, grad_gain = pl.pallas_call(
        place,
        out_shape=(
            jax.ShapeDtypeStruct((ROWS, D), BF16),
            jax.ShapeDtypeStruct((ROWS, D), BF16),
            jax.ShapeDtypeStruct((16, D), F32),
            jax.ShapeDtypeStruct((TAPS, 128), F32),
            jax.ShapeDtypeStruct((1, 128), F32),
        ),
        in_specs=[hbm] * 4,
        out_specs=(hbm,) * 5,
        scratch_shapes=[
            pltpu.VMEM((ROWS, D), BF16),
            pltpu.VMEM((ROWS, D), BF16),
            pltpu.VMEM((16, D), F32),
            pltpu.VMEM((32, 128), F32),
            pltpu.VMEM((TAPS, 128), F32),
            pltpu.VMEM((1, 128), F32),
            pltpu.SemaphoreType.DMA((10,)),
            pltpu.SemaphoreType.DMA((11,)),
        ],
    )(grad_value, grad_gate, grad_weight, grad_taps)
    return (grad_value[None], grad_gate[None], grad_weight, grad_kernel, grad_gain[0])


def solution(mesh):
    placed = (
        P("dp", "sp", None),
        P("dp", "sp", None),
        P("dp", "sp", None),
        P("dp", None),
        P(None, "sp"),
        P("sp"),
    )
    return jax.shard_map(
        shards,
        mesh=mesh,
        in_specs=placed,
        out_specs=(
            P("dp", "sp", None),
            P("dp", "sp", None),
            P(("sp", "dp"), None),
            P(None, "sp"),
            P("sp"),
        ),
        check_vma=False,
    )
```

```python
import functools

import jax
import jax.numpy as jnp
from jax import lax
from jax.experimental import pallas as pl
from jax.experimental.pallas import tpu as pltpu
from jax.sharding import PartitionSpec as P

EPS = 1e-05
F32 = jnp.float32
BF16 = jnp.bfloat16
MESH = pl.DeviceIdType.MESH

ROWS = 256
SEG = 16
D = 2048
HALF = 1024
TAPS = 31
NSP = 16
NDP = 8
WX_COLS, WY_COLS, WZ_COLS = (0, 384), (384, 896), (1280, 768)
COLOURS = ((0, 384), (384, 256), (640, 384))

TAP0 = 0
COT0 = TAP0 + 16
HALO0 = COT0 + 1
WX0 = HALO0 + 2
WY0 = WX0 + 12
WZ0 = WY0 + 12
ACT0 = WZ0 + 12
GA0 = ACT0 + 4
RA0 = GA0 + 4
RB0 = RA0 + 18
RC0 = RB0 + 18
GK0 = RC0 + 21
GD0 = GK0 + 16
GC0 = GD0 + 8
NSEM = GC0 + 1


def sigmoid(x):
    return 0.5 * jnp.tanh(0.5 * x) + 0.5


def lanes(i, n=128):
    return pl.ds(pl.multiple_of(i * n, n), n)


def rows(i, n):
    return pl.ds(pl.multiple_of(i * n, n), n)


def loop(n, body):
    def step(i, c):
        body(i)
        return c

    lax.fori_loop(0, n, step, 0)


def kernel(
    cot_hbm,
    val_hbm,
    gate_hbm,
    w_hbm,
    taps_hbm,
    gain_hbm,
    gv_hbm,
    gg_hbm,
    ow_ref,
    gk_ref,
    cotraw,
    cotp,
    val,
    gate,
    sig,
    gext,
    ext,
    cen,
    fwd,
    act,
    wg,
    ga,
    tkown,
    tkall,
    taps,
    gains,
    sum1,
    sum2,
    inv_b,
    later,
    gcp,
    gcraw,
    ggp,
    gvo,
    ggo,
    gkp,
    gkr,
    gdo,
    gdr,
    pa,
    pb,
    pc,
    r1a,
    r1b,
    r1c,
    cba,
    cbb,
    cbc,
    s1a,
    s1b,
    s1c,
    r2a,
    r2b,
    r2c,
    s2a,
    s2b,
    s2c,
    r3a,
    r3b,
    r3c,
    finp,
    perm,
    taps_in,
    gain_in,
    ssem,
    rsem,
    lsem,
):
    s = lax.axis_index("sp")
    d = lax.axis_index("dp")
    z, y = s // 4, s % 4
    x, q = d // 2, d % 2

    def at(axis, off, core=None):
        dp = d if core is None else x * 2 + core
        if axis == 0:
            return {"sp": s, "dp": ((x + off) % 4) * 2 + (q if core is None else core)}
        if axis == 1:
            return {"sp": z * 4 + (y + off) % 4, "dp": dp}
        return {"sp": ((z + off) % 4) * 4 + y, "dp": dp}

    def slot(axis, off):
        return (off - 1) % 4 if axis == 2 else (coord[axis] + off) % 4

    partner = {"sp": s, "dp": x * 2 + (1 - q)}
    coord = (x, y, z)

    sent = []

    def copy(src, dst, i, dev):
        return pltpu.make_async_remote_copy(
            src_ref=src, dst_ref=dst, send_sem=ssem.at[i], recv_sem=rsem.at[i], device_id=dev, device_id_type=MESH
        )

    def send(src, dst, i, dev):
        c = copy(src, dst, i, dev)
        c.start()
        sent.append(c)

    def got(dst, i):
        copy(dst, dst, i, partner).wait_recv()

    local = [
        pltpu.make_async_copy(w_hbm, wg.at[x], lsem.at[0]),
        pltpu.make_async_copy(val_hbm, val, lsem.at[1]),
        pltpu.make_async_copy(gate_hbm, gate, lsem.at[2]),
        pltpu.make_async_copy(cot_hbm, cotraw.at[q], lsem.at[3]),
    ]
    small = [
        pltpu.make_async_copy(taps_hbm, taps_in, lsem.at[12]),
        pltpu.make_async_copy(gain_hbm, gain_in, lsem.at[13]),
    ]
    for c in (local[0], *small, *local[1:]):
        c.start()
    barrier = pltpu.get_barrier_semaphore()

    def greet_sp(r):
        pl.semaphore_signal(barrier, inc=1, device_id={"sp": (s + r + 1) % NSP, "dp": d}, device_id_type=MESH)

    def greet_dp(r):
        pl.semaphore_signal(barrier, inc=1, device_id={"sp": s, "dp": (d + r + 1) % NDP}, device_id_type=MESH)

    loop(NSP - 1, greet_sp)
    loop(NDP - 1, greet_dp)
    for axis in (1, 2):
        for r in (1, 2, 3):
            pl.semaphore_signal(barrier, inc=1, device_id=at(axis, r, 1 - q), device_id_type=MESH)
    r_io = lax.broadcasted_iota(jnp.int32, (ROWS, ROWS), 0)
    t_io = lax.broadcasted_iota(jnp.int32, (ROWS, ROWS), 1)
    perm[...] = jnp.where(t_io == (r_io & 15) * SEG + (r_io >> 4), 1.0, 0.0).astype(BF16)
    pl.semaphore_wait(barrier, NSP - 1 + NDP - 1 + 6)

    def piece(cols, size):
        def at_quarter(xx, quarter, h=None):
            n, first = (size, quarter * size) if h is None else (size // 2, quarter * size + h * (size // 2))
            return wg.at[xx, pl.ds(pl.multiple_of(first, n), n), pl.ds(*cols)]

        return at_quarter

    wx, wy, wz = piece(WX_COLS, ROWS), piece(WY_COLS, 64), piece(WZ_COLS, 64)

    local[0].wait()
    for i, off in ((0, 1), (1, -1)):
        send(wy(x, y), wy(x, y), WX0 + i, at(0, off))
    for i, off in ((0, 1), (1, -1)):
        send(wz(x, z), wz(x, z), WX0 + 2 + i, at(0, off))

    for c in small:
        c.wait()
    tkown[0:TAPS, :] = taps_in[...].astype(F32)
    tkown[TAPS : TAPS + 1, :] = gain_in[...].astype(F32)
    tkall[s] = tkown[...].astype(BF16)

    def send_taps(r):
        copy(tkall.at[s], tkall.at[s], TAP0 + r, {"sp": (s + r + 1) % NSP, "dp": d}).start()

    loop(NSP - 1, send_taps)

    local[1].wait()
    local[2].wait()

    def gate_block(i):
        at_rows = rows(ROWS // 32 - 1 - i, 32)
        sg = sigmoid(gate[at_rows, :].astype(F32))
        sig[at_rows, :] = sg
        gext[pl.ds(pl.multiple_of((ROWS // 32 - i) * 32, 32), 32), :] = (val[at_rows, :].astype(F32) * sg).astype(BF16)

    gate_block(0)

    def halo_copy(n):
        cols = pl.ds(HALF * n, HALF)
        return copy(
            gext.at[pl.ds(ROWS, 32), cols],
            gext.at[pl.ds(0, 32), cols],
            HALO0 + n,
            {"sp": (s + 1) % NSP, "dp": d},
        )

    @pl.when(s < NSP - 1)
    def _():
        halo_copy(0).start()
        halo_copy(1).start()

    local[3].wait()
    send(cotraw.at[q], cotraw.at[q], COT0, partner)
    loop(ROWS // 32 - 1, lambda i: gate_block(i + 1))

    left, right, far = (x + 3) % 4, (x + 1) % 4, (x + 2) % 4
    both = ((0, 1), (1, -1))

    def along_x(part, quarter, base):
        for i, off in both:
            src = (x - off) % 4
            got(part(src, quarter), WX0 + base + i)
            send(part(src, quarter, i), part(src, quarter, i), WX0 + 6 + base + i, at(0, off))

    def far_along_x(part, quarter, base):
        for i, _ in both:
            got(part(far, quarter, i), WX0 + 6 + base + i)

    def across(axis, xx, pos):
        part, here, base = ((wy, y, WY0), (wz, z, WZ0))[axis - 1]
        for i, off in both:
            send(part(xx, here), part(xx, here), base + 4 * pos + i, at(axis, off))

    def across_on(axis, xx, pos):
        part, here, base = ((wy, y, WY0), (wz, z, WZ0))[axis - 1]
        for i, off in both:
            quarter = (here - off) % 4
            got(part(xx, quarter), base + 4 * pos + i)
            send(part(xx, quarter, i), part(xx, quarter, i), base + 4 * pos + 2 + i, at(axis, off))

    def across_end(axis, xx, pos):
        part, here, base = ((wy, y, WY0), (wz, z, WZ0))[axis - 1]
        for i, _ in both:
            got(part(xx, (here + 2) % 4, i), base + 4 * pos + 2 + i)

    def weights_end(xx, pos):
        across_end(1, xx, pos)
        across_end(2, xx, pos)
        if pos == 2:
            far_along_x(wx, 0, 4)

    def spread_half(src, first, dst, base, n):
        block = jnp.dot(perm[...], src[pl.ds(first, ROWS), lanes(n, HALF)], preferred_element_type=F32)
        block = block.astype(BF16)
        for i in range(8):
            dst[n * 8 + i, pl.ds(base, ROWS), :] = block[:, 128 * i : 128 * i + 128]

    def spread(src, first, dst, base):
        loop(2, lambda n: spread_half(src, first, dst, base, n))

    spread(gext, 32, ext, 2 * ROWS)

    def spread_cot(core):
        def body(n):
            block = jnp.dot(perm[...], cotraw[core, :, lanes(n, 1024)], preferred_element_type=F32)
            cotp[rows(core, ROWS), lanes(n, 1024)] = block.astype(BF16)

        loop(2, body)

    spread_cot(q)
    got(cotraw.at[1 - q], COT0)
    spread_cot(1 - q)

    def halo_in(n):
        cols = pl.ds(HALF * n, HALF)

        @pl.when(s > 0)
        def _():
            got(gext.at[pl.ds(0, 32), cols], HALO0 + n)

        @pl.when(s == 0)
        def _():
            gext[0:32, cols] = jnp.zeros((32, HALF), BF16)

    def spread_before(n):
        spread_half(gext, 16, ext, ROWS, n)
        spread_half(gext, 0, ext, 0, n)

    def got_taps(r):
        src = (s + NSP - 1 - r) % NSP
        got(tkall.at[src], TAP0 + r)

    def widen(i):
        t = tkall[i].astype(F32)
        gains[:, lanes(i)] = jnp.broadcast_to(t[TAPS : TAPS + 1], (16, 128))
        for k in range(TAPS):
            taps[i, 16 * k : 16 * k + 16, :] = jnp.broadcast_to(t[k : k + 1], (16, 128)).astype(BF16)

    def filtered(col, src, shift, emit):
        tiles, weights = src.at[col], taps.at[col]
        for j0 in range(0, SEG, 4):
            acc = [None] * 4
            for k in range(TAPS):
                for o in range(4):
                    at_row = 16 * shift(j0 + o, k)
                    term = weights[16 * k : 16 * k + 16, :].astype(F32) * tiles[at_row : at_row + 16, :].astype(F32)
                    acc[o] = term if acc[o] is None else acc[o] + term
            for o in range(4):
                emit(j0 + o, acc[o])

    def conv_block(col):
        dst = cen.at[col]

        def emit(j, v):
            dst[16 * j : 16 * j + 16, :] = v

        filtered(col, ext, lambda j, k: j - k + 2 * SEG, emit)

    halo_in(0)
    spread_before(0)
    along_x(wy, y, 0)
    across(1, left, 0)
    across(1, right, 1)
    loop(NSP - 1, got_taps)
    loop(NSP, widen)
    loop(8, conv_block)
    along_x(wz, z, 2)
    across(2, left, 0)
    across(2, right, 1)
    for i, off in both:
        send(wx(x, 0), wx(x, 0), WX0 + 4 + i, at(0, off))
    halo_in(1)
    spread_before(1)
    loop(8, lambda i: conv_block(i + 8))


    def conv_sums(j):
        at_rows = rows(j, 16)
        one = two = None
        for col in range(NSP):
            v = cen[col, at_rows, :]
            one = v if one is None else one + v
            two = v * v if two is None else two + v * v
        sum1[at_rows, :] = one
        sum2[at_rows, :] = two

    loop(SEG, conv_sums)
    mean = jnp.sum(sum1[...], axis=1, keepdims=True) * (1.0 / D)
    var = jnp.sum(sum2[...], axis=1, keepdims=True) * (1.0 / D) - mean * mean
    sum1[...] = jnp.broadcast_to(mean, (ROWS, 128))
    inv_b[...] = jnp.broadcast_to(lax.rsqrt(var + EPS), (ROWS, 128))

    def act_block(g, j):
        at_rows = rows(j, 16)
        m, iv = sum1[at_rows, :], inv_b[at_rows, :]
        for i in range(4):
            col = 4 * g + i
            ln = lanes(col)
            centred = (cen[col, at_rows, :] - m) * iv
            cen[col, at_rows, :] = centred
            normed = centred * gains[:, ln]
            sg = sigmoid(normed)
            act[pl.ds(pl.multiple_of(q * ROWS + j * 16, 16), 16), ln] = (normed * sg).astype(BF16)
            fwd[col, at_rows, :] = sg * (1.0 + normed * (1.0 - sg))

    order = (1, 0, 2, 3)
    groups = [(z + 1 + zr) % 4 for zr in order]
    for pos, g in enumerate(groups):
        loop(SEG, lambda j, g=g: act_block(g, j))
        part = act.at[rows(q, ROWS), lanes(g, 512)]
        send(part, part, ACT0 + pos, partner)
        if pos == 2:
            far_along_x(wy, y, 0)
            across(1, far, 2)
        if pos == 3:
            across_on(1, left, 0)
            far_along_x(wz, z, 2)
            across(2, far, 2)

    blocks = (pa, pb, pc)
    half = lanes(q, HALF)

    def outer(g, zr, i):
        p = lax.dot_general(
            act[:, lanes(2 * g + i, 256)], cotp[:, half], (((0,), (0,)), ((), ())), preferred_element_type=F32
        ).astype(BF16)
        for n in range(8):
            yy, xx = i * 2 + n // 4, n % 4
            part = p[32 * n : 32 * n + 32]
            pa[xx, yy, zr] = part[:, 0:384]
            pb[yy, zr, xx] = part[:, 384:640]
            pc[zr, xx, yy] = part[:, 640:1024]

    r1s, cbs = (r1a, r1b, r1c), (cba, cbb, cbc)
    s1s, r2s, s2s, r3s = (s1a, s1b, s1c), (r2a, r2b, r2c), (s2a, s2b, s2c), (r3a, r3b, r3c)
    firsts, lasts = pl.ds(0, 2), pl.ds(2, 2)

    def half_of(c, off, h):
        cut = (firsts, lasts)[h]
        if c == 1:
            return blocks[c].at[slot(c, off), cut]
        return blocks[c].at[slot(c, off), :, cut]

    def sums_far(c, h):
        send(half_of(c, 2, h), r1s[c].at[h], RA0 + 6 * c + h, at(c, (1, -1)[h]))

    def sums_alone(c, h):
        send(half_of(c, (-1, 1)[h], h), r1s[c].at[3 - h], RA0 + 6 * c + 3 - h, at(c, (-1, 1)[h]))

    for pos, (g, zr) in enumerate(zip(groups, order)):
        got(act.at[rows(1 - q, ROWS), lanes(g, 512)], ACT0 + pos)
        loop(2, lambda i, g=g, zr=zr: outer(g, zr, i))
        if pos == 1:
            across_on(2, left, 0)
            across_on(1, right, 1)
            sums_far(0, 0)
            sums_alone(0, 0)
        if pos == 2:
            across_on(2, right, 1)
        if pos == 3:
            along_x(wx, 0, 4)
            sums_far(0, 1)
            across_on(1, far, 2)
            sums_far(1, 0)
            sums_far(1, 1)
            across_on(2, far, 2)
            sums_far(2, 0)
            sums_far(2, 1)
            for c in (2, 1):
                sums_alone(c, 0)
                sums_alone(c, 1)
            sums_alone(0, 1)

    def each(c, body):
        loop(8, (lambda i: body(i // 4, i % 4)) if c == 1 else (lambda i: body(i // 2, i % 2)))

    def join(c, h):
        got(r1s[c].at[h], RA0 + 6 * c + h)
        own = half_of(c, (1, -1)[h], h)

        def add(a, b):
            cbs[c][h, a, b] = (own[a, b].astype(F32) + r1s[c][h, a, b].astype(F32)).astype(BF16)

        each(c, add)
        send(cbs[c].at[h], r1s[c].at[4 + h], RA0 + 6 * c + 4 + h, at(c, (1, -1)[h]))

    def back_send(pos, xx):
        blk = xx * 2 + q
        g = lax.dot_general(cotp[...], wg[xx], (((1,), (1,)), ((), ())), preferred_element_type=F32).astype(BF16)
        finp[pos] = g
        ga[blk] = finp[pos, rows(q, ROWS), :]
        send(finp.at[pos, rows(1 - q, ROWS)], ga.at[blk], GA0 + pos, partner)

    back_send(3, x)
    weights_end(left, 0)
    back_send(0, left)
    weights_end(right, 1)
    back_send(1, right)
    join(0, 0)
    weights_end(far, 2)
    back_send(2, far)

    join(1, 0)
    join(1, 1)
    join(2, 0)
    join(2, 1)
    join(0, 1)

    for pos, off in ((3, 0), (0, 3), (1, 1), (2, 2)):
        got(ga.at[((x + off) % 4) * 2 + 1 - q], GA0 + pos)

    def grad_block(j, gsums):
        at_rows = rows(j, 16)
        one = two = None
        out_sums = []
        for col in range(NSP):
            ln = pl.ds(128 * col, 128)
            gn = ga[col // 2, at_rows, pl.ds(128 * (col % 2), 128)].astype(F32) * fwd[col, at_rows, :]
            prod = gn * cen[col, at_rows, :]
            out_sums.append(gsums[col] + prod[0:8] + prod[8:16])
            gain = gains[:, ln]
            gc = gn * gain
            fwd[col, at_rows, :] = gc
            prod = prod * gain
            one = gc if one is None else one + gc
            two = prod if two is None else two + prod
        sum1[at_rows, :] = one
        sum2[at_rows, :] = two
        return out_sums

    gsums = lax.fori_loop(0, SEG, grad_block, [jnp.zeros((8, 128), F32)] * NSP)
    for col in range(NSP):
        gkp[col, TAPS : TAPS + 1, :] = jnp.sum(gsums[col], axis=0, keepdims=True)
    m1 = jnp.sum(sum1[...], axis=1, keepdims=True) * (1.0 / D)
    m2 = jnp.sum(sum2[...], axis=1, keepdims=True) * (1.0 / D)
    sum1[...] = jnp.broadcast_to(m1, (ROWS, 128))
    sum2[...] = jnp.broadcast_to(m2, (ROWS, 128))

    def norm_block(j):
        at_rows = rows(j, 16)
        a, b, iv = sum1[at_rows, :], sum2[at_rows, :], inv_b[at_rows, :]
        for col in range(NSP):
            v = ((fwd[col, at_rows, :] - a - cen[col, at_rows, :] * b) * iv).astype(BF16)
            later[col, at_rows, :] = v
            gcp[at_rows, pl.ds(128 * col, 128)] = v

    loop(SEG, norm_block)

    def in_order(n):
        block = jnp.dot(perm[...], gcp[:, lanes(n, 1024)], preferred_element_type=F32)
        gcraw[0:ROWS, lanes(n, 1024)] = block.astype(BF16)

    loop(2, in_order)

    def margin_copy():
        return copy(
            gcraw.at[pl.ds(0, 32)], gcraw.at[pl.ds(ROWS, 32)], GC0, {"sp": (s + NSP - 1) % NSP, "dp": d}
        )

    @pl.when(s > 0)
    def _():
        margin_copy().start()

    def tap_block(col):
        grads, tiles, sums = later.at[col], ext.at[col], gkp.at[col]
        for k0 in range(0, TAPS, 4):
            taps_here = range(k0, min(k0 + 4, TAPS))
            acc = {}
            for j in range(SEG):
                for k in taps_here:
                    at_row = 16 * (j - k + 2 * SEG)
                    term = grads[16 * j : 16 * j + 16, :].astype(F32) * tiles[at_row : at_row + 16, :].astype(F32)
                    acc[k] = term if j == 0 else acc[k] + term
            for k in taps_here:
                sums[k : k + 1, :] = jnp.sum(acc[k][0:8] + acc[k][8:16], axis=0, keepdims=True)

    loop(NSP, tap_block)

    def send_gk(r):
        dst = (s + r + 1) % NSP
        copy(gkp.at[dst], gkr.at[r], GK0 + r, {"sp": dst, "dp": d}).start()

    loop(NSP - 1, send_gk)

    def stage1(c, h):
        pair = ((4, 3), (2, 5))[h]
        for n in pair:
            got(r1s[c].at[n], RA0 + 6 * c + n)
        own, cut = half_of(c, 0, h), (firsts, lasts)[h]
        dst = s1s[c].at[cut] if c == 1 else s1s[c].at[:, cut]

        def add(a, b):
            dst[a, b] = (
                own[a, b].astype(F32) + r1s[c][pair[0], a, b].astype(F32) + r1s[c][pair[1], a, b].astype(F32)
            ).astype(BF16)

        each(c, add)
        axis = (c + 1) % 3
        for r in (2, 1, 3):
            i = slot(axis, r)
            if c != 1:
                send(s1s[c].at[i, cut], r2s[c].at[r - 1, cut], RB0 + 6 * c + 2 * (r - 1) + h, at(axis, r))
            elif i // 2 == h:
                send(s1s[c].at[i], r2s[c].at[r - 1], RB0 + 6 * c + 2 * (r - 1), at(axis, r))

    def stage2(c):
        axis, last = (c + 1) % 3, (c + 2) % 3
        for r in range(1, 4):
            if c == 1:
                got(r2s[c].at[r - 1], RB0 + 6 * c + 2 * (r - 1))
            else:
                for h, cut in enumerate((firsts, lasts)):
                    got(r2s[c].at[r - 1, cut], RB0 + 6 * c + 2 * (r - 1) + h)

        def add(i):
            total = s1s[c][slot(axis, 0), i].astype(F32)
            for r in range(3):
                total = total + r2s[c][r, i].astype(F32)
            s2s[c][i] = total.astype(BF16)

        loop(4, add)
        for r in (2, 1, 3):
            for other in range(2):
                core = 1 - q if other else q
                send(
                    s2s[c].at[slot(last, r), rows(core, 16)],
                    r3s[c].at[other, r],
                    RC0 + 7 * c + 2 * r + other - 1,
                    at(last, r, core),
                )
        send(s2s[c].at[slot(last, 0), rows(1 - q, 16)], r3s[c].at[1, 0], RC0 + 7 * c, partner)

    factor = float(NSP * NDP * ROWS) ** (-0.5)

    def stage3(c):
        last = (c + 2) % 3
        first, size = COLOURS[c]
        got(r3s[c].at[1, 0], RC0 + 7 * c)
        for r in range(1, 4):
            for other in range(2):
                got(r3s[c].at[other, r], RC0 + 7 * c + 2 * r + other - 1)
        for other in range(2):
            if other:
                total = r3s[c][1, 0].astype(F32)
            else:
                total = s2s[c][slot(last, 0), rows(q, 16), :].astype(F32)
            for r in range(1, 4):
                total = total + r3s[c][other, r].astype(F32)
            core = 1 - q if other else q
            ow_ref[:, pl.ds(pl.multiple_of(core * HALF + first, 128), size)] = total * factor

    for c in (1, 0, 2):
        for h in range(2):
            stage1(c, h)

    @pl.when(s < NSP - 1)
    def _():
        got(gcraw.at[pl.ds(ROWS, 32)], GC0)

    @pl.when(s == NSP - 1)
    def _():
        gcraw[ROWS : ROWS + 32, :] = jnp.zeros((32, D), BF16)

    spread(gcraw, 16, later, ROWS)
    spread(gcraw, 32, later, 2 * ROWS)

    def back_block(col):
        ln = lanes(col)

        def emit(j, v):
            ggp[16 * j : 16 * j + 16, ln] = v.astype(BF16)

        filtered(col, later, lambda j, k: j + k, emit)

    out = []

    def finish(g):
        cols = pl.ds(512 * g, 512)
        grad = jnp.dot(perm[...], ggp[:, cols], preferred_element_type=F32)
        sg = sig[:, cols]
        gvo[:, cols] = (grad * sg).astype(BF16)
        ggo[:, cols] = (grad * val[:, cols].astype(F32) * sg * (1.0 - sg)).astype(BF16)
        for c in (
            pltpu.make_async_copy(gvo.at[:, cols], gv_hbm.at[:, cols], lsem.at[4 + 2 * g]),
            pltpu.make_async_copy(ggo.at[:, cols], gg_hbm.at[:, cols], lsem.at[5 + 2 * g]),
        ):
            c.start()
            out.append(c)

    def group(g):
        loop(4, lambda i: back_block(i + 4 * g))
        finish(g)

    group(0)

    group(1)
    def got_gk(r):
        got(gkr.at[r], GK0 + r)

    loop(NSP - 1, got_gk)
    total = gkp[s]
    for r in range(NSP - 1):
        total = total + gkr[r]
    gdo[...] = total

    def send_gd(r):
        copy(gdo, gdr.at[r], GD0 + r, {"sp": s, "dp": (d + r + 1) % NDP}).start()

    loop(NDP - 1, send_gd)
    group(2)
    group(3)
    for c in (1, 0, 2):
        stage2(c)
    for c in (1, 0, 2):
        stage3(c)

    def got_gd(r):
        got(gdr.at[r], GD0 + r)

    loop(NDP - 1, got_gd)
    total = gdo[...]
    for r in range(NDP - 1):
        total = total + gdr[r]
    gk_ref[...] = total * factor

    for c in sent:
        c.wait_send()

    def drain_sp(r):
        copy(tkall.at[s], tkall.at[s], TAP0 + r, partner).wait_send()
        copy(gkp.at[s], gkr.at[r], GK0 + r, partner).wait_send()

    loop(NSP - 1, drain_sp)

    def drain_dp(r):
        copy(gdo, gdr.at[r], GD0 + r, partner).wait_send()

    loop(NDP - 1, drain_dp)

    @pl.when(s < NSP - 1)
    def _():
        halo_copy(0).wait_send()
        halo_copy(1).wait_send()

    @pl.when(s > 0)
    def _():
        margin_copy().wait_send()

    for c in out:
        c.wait()


def place(gv_in, gg_in, ow_in, gk_in, gv_hbm, gg_hbm, ow_hbm, taps_hbm, gain_hbm, gv, gg, ow, gk, tp, gn, lsem, ssem):
    ins, outs = [], []
    for i in range(4):
        at_rows = pl.ds(64 * i, 64)
        ins.append(pltpu.make_async_copy(gv_in.at[at_rows], gv.at[at_rows], lsem.at[2 * i]))
        outs.append(pltpu.make_async_copy(gv.at[at_rows], gv_hbm.at[at_rows], ssem.at[2 * i]))
        ins.append(pltpu.make_async_copy(gg_in.at[at_rows], gg.at[at_rows], lsem.at[2 * i + 1]))
        outs.append(pltpu.make_async_copy(gg.at[at_rows], gg_hbm.at[at_rows], ssem.at[2 * i + 1]))
    ins.append(pltpu.make_async_copy(ow_in, ow, lsem.at[8]))
    outs.append(pltpu.make_async_copy(ow, ow_hbm, ssem.at[8]))
    small = pltpu.make_async_copy(gk_in, gk, lsem.at[9])
    small.start()
    for c in ins:
        c.start()
    for c, o in zip(ins, outs):
        c.wait()
        o.start()
    small.wait()
    tp[...] = gk[0:TAPS, :]
    gn[...] = gk[TAPS : TAPS + 1, :]
    outs.append(pltpu.make_async_copy(tp, taps_hbm, ssem.at[9]))
    outs.append(pltpu.make_async_copy(gn, gain_hbm, ssem.at[10]))
    outs[-2].start()
    outs[-1].start()
    for o in outs:
        o.wait()


def shards(out_cotangent, value_pre, gate_pre, out_weight, conv_kernel, norm_gain):
    hbm = pl.BlockSpec(memory_space=pl.ANY)
    vmem = pl.BlockSpec(memory_space=pltpu.VMEM)
    sizes = [size for _, size in COLOURS]
    scratch = [
        ((2, ROWS, D), BF16),
        ((2 * ROWS, D), BF16),
        ((ROWS, D), BF16),
        ((ROWS, D), BF16),
        ((ROWS, D), F32),
        ((ROWS + 32, D), BF16),
        ((NSP, 3 * ROWS, 128), BF16),
        ((NSP, ROWS, 128), F32),
        ((NSP, ROWS, 128), F32),
        ((2 * ROWS, D), BF16),
        ((4, ROWS, D), BF16),
        ((8, ROWS, ROWS), BF16),
        ((32, 128), F32),
        ((NSP, 32, 128), BF16),
        ((NSP, 16 * TAPS, 128), BF16),
        ((16, D), F32),
        ((ROWS, 128), F32),
        ((ROWS, 128), F32),
        ((ROWS, 128), F32),
        ((NSP, 3 * ROWS, 128), BF16),
        ((ROWS, D), BF16),
        ((ROWS + 32, D), BF16),
        ((ROWS, D), BF16),
        ((ROWS, D), BF16),
        ((ROWS, D), BF16),
        ((NSP, 32, 128), F32),
        ((NSP - 1, 32, 128), F32),
        ((32, 128), F32),
        ((NDP - 1, 32, 128), F32),
    ]
    scratch += [((4, 4, 4, 32, f), BF16) for f in sizes]
    halves = [(4, 2), (2, 4), (4, 2)]
    scratch += [((6, *h, 32, f), BF16) for h, f in zip(halves, sizes)]
    scratch += [((2, *h, 32, f), BF16) for h, f in zip(halves, sizes)]
    scratch += [((4, 4, 32, f), BF16) for f in sizes]
    scratch += [((3, 4, 32, f), BF16) for f in sizes]
    scratch += [((4, 32, f), BF16) for f in sizes]
    scratch += [((2, 4, 16, f), BF16) for f in sizes]
    scratch += [
        ((4, 2 * ROWS, ROWS), BF16),
        ((ROWS, ROWS), BF16),
        ((TAPS, 128), BF16),
        ((1, 128), BF16),
    ]
    grad_value, grad_gate, grad_weight, grad_taps = pl.pallas_call(
        kernel,
        out_shape=(
            jax.ShapeDtypeStruct((ROWS, D), BF16),
            jax.ShapeDtypeStruct((ROWS, D), BF16),
            jax.ShapeDtypeStruct((16, D), F32),
            jax.ShapeDtypeStruct((32, 128), F32),
        ),
        in_specs=[pl.BlockSpec(memory_space=pltpu.HBM)] * 6,
        out_specs=(hbm, hbm, vmem, vmem),
        scratch_shapes=[pltpu.VMEM(shape, kind) for shape, kind in scratch]
        + [pltpu.SemaphoreType.DMA((NSEM,)), pltpu.SemaphoreType.DMA((NSEM,)), pltpu.SemaphoreType.DMA((14,))],
        compiler_params=pltpu.CompilerParams(
            collective_id=0, has_side_effects=True, vmem_limit_bytes=60 * 1024 * 1024
        ),
    )(out_cotangent[0], value_pre[0], gate_pre[0], out_weight, conv_kernel, norm_gain[None])
    grad_value, grad_gate, grad_weight, grad_kernel, grad_gain = pl.pallas_call(
        place,
        out_shape=(
            jax.ShapeDtypeStruct((ROWS, D), BF16),
            jax.ShapeDtypeStruct((ROWS, D), BF16),
            jax.ShapeDtypeStruct((16, D), F32),
            jax.ShapeDtypeStruct((TAPS, 128), F32),
            jax.ShapeDtypeStruct((1, 128), F32),
        ),
        in_specs=[hbm] * 4,
        out_specs=(hbm,) * 5,
        scratch_shapes=[
            pltpu.VMEM((ROWS, D), BF16),
            pltpu.VMEM((ROWS, D), BF16),
            pltpu.VMEM((16, D), F32),
            pltpu.VMEM((32, 128), F32),
            pltpu.VMEM((TAPS, 128), F32),
            pltpu.VMEM((1, 128), F32),
            pltpu.SemaphoreType.DMA((10,)),
            pltpu.SemaphoreType.DMA((11,)),
        ],
    )(grad_value, grad_gate, grad_weight, grad_taps)
    return (grad_value[None], grad_gate[None], grad_weight, grad_kernel, grad_gain[0])


def solution(mesh):
    placed = (
        P("dp", "sp", None),
        P("dp", "sp", None),
        P("dp", "sp", None),
        P("dp", None),
        P(None, "sp"),
        P("sp"),
    )
    return jax.shard_map(
        shards,
        mesh=mesh,
        in_specs=placed,
        out_specs=(
            P("dp", "sp", None),
            P("dp", "sp", None),
            P(("sp", "dp"), None),
            P(None, "sp"),
            P("sp"),
        ),
        check_vma=False,
    )
```

```python
import functools

import jax
import jax.numpy as jnp
from jax import lax
from jax.experimental import pallas as pl
from jax.experimental.pallas import tpu as pltpu
from jax.sharding import PartitionSpec as P

EPS = 1e-05
F32 = jnp.float32
BF16 = jnp.bfloat16
MESH = pl.DeviceIdType.MESH

ROWS = 256
SEG = 16
D = 2048
HALF = 1024
TAPS = 31
NSP = 16
NDP = 8
WX_COLS, WY_COLS, WZ_COLS = (0, 384), (384, 896), (1280, 768)
COLOURS = ((0, 384), (384, 256), (640, 384))

TAP0 = 0
COT0 = TAP0 + 16
HALO0 = COT0 + 1
WX0 = HALO0 + 2
WY0 = WX0 + 12
WZ0 = WY0 + 12
ACT0 = WZ0 + 12
GA0 = ACT0 + 4
RA0 = GA0 + 4
RB0 = RA0 + 18
RC0 = RB0 + 18
GK0 = RC0 + 21
GD0 = GK0 + 16
GC0 = GD0 + 8
NSEM = GC0 + 1


def sigmoid(x):
    return 0.5 * jnp.tanh(0.5 * x) + 0.5


def lanes(i, n=128):
    return pl.ds(pl.multiple_of(i * n, n), n)


def rows(i, n):
    return pl.ds(pl.multiple_of(i * n, n), n)


def loop(n, body):
    def step(i, c):
        body(i)
        return c

    lax.fori_loop(0, n, step, 0)


def kernel(
    cot_hbm,
    val_hbm,
    gate_hbm,
    w_hbm,
    taps_hbm,
    gain_hbm,
    gv_hbm,
    gg_hbm,
    ow_ref,
    gk_ref,
    cotraw,
    cotp,
    val,
    gate,
    sig,
    gext,
    ext,
    cen,
    fwd,
    act,
    wg,
    ga,
    tkown,
    tkall,
    taps,
    gains,
    sum1,
    sum2,
    inv_b,
    later,
    gcp,
    gcraw,
    ggp,
    gvo,
    ggo,
    gkp,
    gkr,
    gdo,
    gdr,
    pa,
    pb,
    pc,
    r1a,
    r1b,
    r1c,
    cba,
    cbb,
    cbc,
    s1a,
    s1b,
    s1c,
    r2a,
    r2b,
    r2c,
    s2a,
    s2b,
    s2c,
    r3a,
    r3b,
    r3c,
    finp,
    perm,
    taps_in,
    gain_in,
    ssem,
    rsem,
    lsem,
):
    s = lax.axis_index("sp")
    d = lax.axis_index("dp")
    z, y = s // 4, s % 4
    x, q = d // 2, d % 2

    def at(axis, off, core=None):
        dp = d if core is None else x * 2 + core
        if axis == 0:
            return {"sp": s, "dp": ((x + off) % 4) * 2 + (q if core is None else core)}
        if axis == 1:
            return {"sp": z * 4 + (y + off) % 4, "dp": dp}
        return {"sp": ((z + off) % 4) * 4 + y, "dp": dp}

    def slot(axis, off):
        return (off - 1) % 4 if axis == 2 else (coord[axis] + off) % 4

    partner = {"sp": s, "dp": x * 2 + (1 - q)}
    coord = (x, y, z)

    sent = []

    def copy(src, dst, i, dev):
        return pltpu.make_async_remote_copy(
            src_ref=src, dst_ref=dst, send_sem=ssem.at[i], recv_sem=rsem.at[i], device_id=dev, device_id_type=MESH
        )

    def send(src, dst, i, dev):
        c = copy(src, dst, i, dev)
        c.start()
        sent.append(c)

    def got(dst, i):
        copy(dst, dst, i, partner).wait_recv()

    local = [
        pltpu.make_async_copy(w_hbm, wg.at[x], lsem.at[0]),
        pltpu.make_async_copy(val_hbm, val, lsem.at[1]),
        pltpu.make_async_copy(gate_hbm, gate, lsem.at[2]),
        pltpu.make_async_copy(cot_hbm, cotraw.at[q], lsem.at[3]),
    ]
    small = [
        pltpu.make_async_copy(taps_hbm, taps_in, lsem.at[12]),
        pltpu.make_async_copy(gain_hbm, gain_in, lsem.at[13]),
    ]
    for c in (local[0], *small, *local[1:]):
        c.start()
    barrier = pltpu.get_barrier_semaphore()

    def greet_sp(r):
        pl.semaphore_signal(barrier, inc=1, device_id={"sp": (s + r + 1) % NSP, "dp": d}, device_id_type=MESH)

    def greet_dp(r):
        pl.semaphore_signal(barrier, inc=1, device_id={"sp": s, "dp": (d + r + 1) % NDP}, device_id_type=MESH)

    loop(NSP - 1, greet_sp)
    loop(NDP - 1, greet_dp)
    for axis in (1, 2):
        for r in (1, 2, 3):
            pl.semaphore_signal(barrier, inc=1, device_id=at(axis, r, 1 - q), device_id_type=MESH)
    r_io = lax.broadcasted_iota(jnp.int32, (ROWS, ROWS), 0)
    t_io = lax.broadcasted_iota(jnp.int32, (ROWS, ROWS), 1)
    perm[...] = jnp.where(t_io == (r_io & 15) * SEG + (r_io >> 4), 1.0, 0.0).astype(BF16)
    local[1].wait()
    local[2].wait()

    def gate_block(i):
        at_rows = rows(ROWS // 32 - 1 - i, 32)
        sg = sigmoid(gate[at_rows, :].astype(F32))
        sig[at_rows, :] = sg
        gext[pl.ds(pl.multiple_of((ROWS // 32 - i) * 32, 32), 32), :] = (val[at_rows, :].astype(F32) * sg).astype(BF16)

    gate_block(0)

    def halo_copy(n):
        cols = pl.ds(HALF * n, HALF)
        return copy(
            gext.at[pl.ds(ROWS, 32), cols],
            gext.at[pl.ds(0, 32), cols],
            HALO0 + n,
            {"sp": (s + 1) % NSP, "dp": d},
        )
    pl.semaphore_wait(barrier, NSP - 1 + NDP - 1 + 6)

    def piece(cols, size):
        def at_quarter(xx, quarter, h=None):
            n, first = (size, quarter * size) if h is None else (size // 2, quarter * size + h * (size // 2))
            return wg.at[xx, pl.ds(pl.multiple_of(first, n), n), pl.ds(*cols)]

        return at_quarter

    wx, wy, wz = piece(WX_COLS, ROWS), piece(WY_COLS, 64), piece(WZ_COLS, 64)

    local[0].wait()
    for i, off in ((0, 1), (1, -1)):
        send(wy(x, y), wy(x, y), WX0 + i, at(0, off))
    for i, off in ((0, 1), (1, -1)):
        send(wz(x, z), wz(x, z), WX0 + 2 + i, at(0, off))

    @pl.when(s < NSP - 1)
    def _():
        halo_copy(0).start()

    for c in small:
        c.wait()
    tkown[0:TAPS, :] = taps_in[...].astype(F32)
    tkown[TAPS : TAPS + 1, :] = gain_in[...].astype(F32)
    tkall[s] = tkown[...].astype(BF16)

    def send_taps(r):
        copy(tkall.at[s], tkall.at[s], TAP0 + r, {"sp": (s + r + 1) % NSP, "dp": d}).start()

    loop(NSP - 1, send_taps)

    @pl.when(s < NSP - 1)
    def _():
        halo_copy(1).start()

    local[3].wait()
    send(cotraw.at[q], cotraw.at[q], COT0, partner)
    loop(ROWS // 32 - 1, lambda i: gate_block(i + 1))

    left, right, far = (x + 3) % 4, (x + 1) % 4, (x + 2) % 4
    both = ((0, 1), (1, -1))

    def along_x(part, quarter, base):
        for i, off in both:
            src = (x - off) % 4
            got(part(src, quarter), WX0 + base + i)
            send(part(src, quarter, i), part(src, quarter, i), WX0 + 6 + base + i, at(0, off))

    def far_along_x(part, quarter, base):
        for i, _ in both:
            got(part(far, quarter, i), WX0 + 6 + base + i)

    def across(axis, xx, pos):
        part, here, base = ((wy, y, WY0), (wz, z, WZ0))[axis - 1]
        for i, off in both:
            send(part(xx, here), part(xx, here), base + 4 * pos + i, at(axis, off))

    def across_on(axis, xx, pos):
        part, here, base = ((wy, y, WY0), (wz, z, WZ0))[axis - 1]
        for i, off in both:
            quarter = (here - off) % 4
            got(part(xx, quarter), base + 4 * pos + i)
            send(part(xx, quarter, i), part(xx, quarter, i), base + 4 * pos + 2 + i, at(axis, off))

    def across_end(axis, xx, pos):
        part, here, base = ((wy, y, WY0), (wz, z, WZ0))[axis - 1]
        for i, _ in both:
            got(part(xx, (here + 2) % 4, i), base + 4 * pos + 2 + i)

    def weights_end(xx, pos):
        across_end(1, xx, pos)
        across_end(2, xx, pos)
        if pos == 2:
            far_along_x(wx, 0, 4)

    def spread_half(src, first, dst, base, n):
        block = jnp.dot(perm[...], src[pl.ds(first, ROWS), lanes(n, HALF)], preferred_element_type=F32)
        block = block.astype(BF16)
        for i in range(8):
            dst[n * 8 + i, pl.ds(base, ROWS), :] = block[:, 128 * i : 128 * i + 128]

    def spread(src, first, dst, base):
        loop(2, lambda n: spread_half(src, first, dst, base, n))

    spread(gext, 32, ext, 2 * ROWS)

    def spread_cot(core):
        def body(n):
            block = jnp.dot(perm[...], cotraw[core, :, lanes(n, 1024)], preferred_element_type=F32)
            cotp[rows(core, ROWS), lanes(n, 1024)] = block.astype(BF16)

        loop(2, body)

    spread_cot(q)
    got(cotraw.at[1 - q], COT0)
    spread_cot(1 - q)

    def halo_in(n):
        cols = pl.ds(HALF * n, HALF)

        @pl.when(s > 0)
        def _():
            got(gext.at[pl.ds(0, 32), cols], HALO0 + n)

        @pl.when(s == 0)
        def _():
            gext[0:32, cols] = jnp.zeros((32, HALF), BF16)

    def spread_before(n):
        spread_half(gext, 16, ext, ROWS, n)
        spread_half(gext, 0, ext, 0, n)

    def got_taps(r):
        src = (s + NSP - 1 - r) % NSP
        got(tkall.at[src], TAP0 + r)

    def widen(i):
        t = tkall[i].astype(F32)
        gains[:, lanes(i)] = jnp.broadcast_to(t[TAPS : TAPS + 1], (16, 128))
        for k in range(TAPS):
            taps[i, 16 * k : 16 * k + 16, :] = jnp.broadcast_to(t[k : k + 1], (16, 128)).astype(BF16)

    def filtered(col, src, shift, emit):
        tiles, weights = src.at[col], taps.at[col]
        for j0 in range(0, SEG, 4):
            acc = [None] * 4
            for k in range(TAPS):
                for o in range(4):
                    at_row = 16 * shift(j0 + o, k)
                    term = weights[16 * k : 16 * k + 16, :].astype(F32) * tiles[at_row : at_row + 16, :].astype(F32)
                    acc[o] = term if acc[o] is None else acc[o] + term
            for o in range(4):
                emit(j0 + o, acc[o])

    def conv_block(col):
        dst = cen.at[col]

        def emit(j, v):
            dst[16 * j : 16 * j + 16, :] = v

        filtered(col, ext, lambda j, k: j - k + 2 * SEG, emit)

    halo_in(0)
    spread_before(0)
    along_x(wy, y, 0)
    across(1, left, 0)
    across(1, right, 1)
    loop(NSP - 1, got_taps)
    loop(NSP, widen)
    loop(8, conv_block)
    along_x(wz, z, 2)
    across(2, left, 0)
    across(2, right, 1)
    for i, off in both:
        send(wx(x, 0), wx(x, 0), WX0 + 4 + i, at(0, off))
    halo_in(1)
    spread_before(1)
    loop(8, lambda i: conv_block(i + 8))


    def conv_sums(j):
        at_rows = rows(j, 16)
        one = two = None
        for col in range(NSP):
            v = cen[col, at_rows, :]
            one = v if one is None else one + v
            two = v * v if two is None else two + v * v
        sum1[at_rows, :] = one
        sum2[at_rows, :] = two

    loop(SEG, conv_sums)
    mean = jnp.sum(sum1[...], axis=1, keepdims=True) * (1.0 / D)
    var = jnp.sum(sum2[...], axis=1, keepdims=True) * (1.0 / D) - mean * mean
    sum1[...] = jnp.broadcast_to(mean, (ROWS, 128))
    inv_b[...] = jnp.broadcast_to(lax.rsqrt(var + EPS), (ROWS, 128))

    def act_block(g, j):
        at_rows = rows(j, 16)
        m, iv = sum1[at_rows, :], inv_b[at_rows, :]
        for i in range(4):
            col = 4 * g + i
            ln = lanes(col)
            centred = (cen[col, at_rows, :] - m) * iv
            cen[col, at_rows, :] = centred
            normed = centred * gains[:, ln]
            sg = sigmoid(normed)
            act[pl.ds(pl.multiple_of(q * ROWS + j * 16, 16), 16), ln] = (normed * sg).astype(BF16)
            fwd[col, at_rows, :] = sg * (1.0 + normed * (1.0 - sg))

    order = (1, 0, 2, 3)
    groups = [(z + 1 + zr) % 4 for zr in order]
    for pos, g in enumerate(groups):
        loop(SEG, lambda j, g=g: act_block(g, j))
        part = act.at[rows(q, ROWS), lanes(g, 512)]
        send(part, part, ACT0 + pos, partner)
        if pos == 2:
            far_along_x(wy, y, 0)
            across(1, far, 2)
        if pos == 3:
            across_on(1, left, 0)
            far_along_x(wz, z, 2)
            across(2, far, 2)

    blocks = (pa, pb, pc)
    half = lanes(q, HALF)

    def outer(g, zr):
        p = lax.dot_general(
            act[:, lanes(g, 512)], cotp[:, half], (((0,), (0,)), ((), ())), preferred_element_type=F32
        ).astype(BF16)
        for n in range(16):
            yy, xx = n // 4, n % 4
            part = p[32 * n : 32 * n + 32]
            pa[xx, yy, zr] = part[:, 0:384]
            pb[yy, zr, xx] = part[:, 384:640]
            pc[zr, xx, yy] = part[:, 640:1024]

    r1s, cbs = (r1a, r1b, r1c), (cba, cbb, cbc)
    s1s, r2s, s2s, r3s = (s1a, s1b, s1c), (r2a, r2b, r2c), (s2a, s2b, s2c), (r3a, r3b, r3c)
    firsts, lasts = pl.ds(0, 2), pl.ds(2, 2)

    def half_of(c, off, h):
        cut = (firsts, lasts)[h]
        if c == 1:
            return blocks[c].at[slot(c, off), cut]
        return blocks[c].at[slot(c, off), :, cut]

    def sums_far(c, h):
        send(half_of(c, 2, h), r1s[c].at[h], RA0 + 6 * c + h, at(c, (1, -1)[h]))

    def sums_alone(c, h):
        send(half_of(c, (-1, 1)[h], h), r1s[c].at[3 - h], RA0 + 6 * c + 3 - h, at(c, (-1, 1)[h]))

    for pos, (g, zr) in enumerate(zip(groups, order)):
        got(act.at[rows(1 - q, ROWS), lanes(g, 512)], ACT0 + pos)
        outer(g, zr)
        if pos == 1:
            across_on(2, left, 0)
            across_on(1, right, 1)
            sums_far(0, 0)
            sums_alone(0, 0)
        if pos == 2:
            across_on(2, right, 1)
        if pos == 3:
            along_x(wx, 0, 4)
            sums_far(0, 1)
            across_on(1, far, 2)
            sums_far(1, 0)
            sums_far(1, 1)
            across_on(2, far, 2)
            sums_far(2, 0)
            sums_far(2, 1)
            for c in (2, 1):
                sums_alone(c, 0)
                sums_alone(c, 1)
            sums_alone(0, 1)

    def each(c, body):
        loop(8, (lambda i: body(i // 4, i % 4)) if c == 1 else (lambda i: body(i // 2, i % 2)))

    def join(c, h):
        got(r1s[c].at[h], RA0 + 6 * c + h)
        own = half_of(c, (1, -1)[h], h)

        def add(a, b):
            cbs[c][h, a, b] = (own[a, b].astype(F32) + r1s[c][h, a, b].astype(F32)).astype(BF16)

        each(c, add)
        send(cbs[c].at[h], r1s[c].at[4 + h], RA0 + 6 * c + 4 + h, at(c, (1, -1)[h]))

    def back_send(pos, xx):
        blk = xx * 2 + q
        g = lax.dot_general(cotp[...], wg[xx], (((1,), (1,)), ((), ())), preferred_element_type=F32).astype(BF16)
        finp[pos] = g
        ga[blk] = finp[pos, rows(q, ROWS), :]
        send(finp.at[pos, rows(1 - q, ROWS)], ga.at[blk], GA0 + pos, partner)

    back_send(3, x)
    weights_end(left, 0)
    back_send(0, left)
    weights_end(right, 1)
    back_send(1, right)
    join(0, 0)
    weights_end(far, 2)
    back_send(2, far)

    join(1, 0)
    join(1, 1)
    join(2, 0)
    join(2, 1)
    join(0, 1)

    for pos, off in ((3, 0), (0, 3), (1, 1), (2, 2)):
        got(ga.at[((x + off) % 4) * 2 + 1 - q], GA0 + pos)

    def grad_block(j, gsums):
        at_rows = rows(j, 16)
        one = two = None
        out_sums = []
        for col in range(NSP):
            ln = pl.ds(128 * col, 128)
            gn = ga[col // 2, at_rows, pl.ds(128 * (col % 2), 128)].astype(F32) * fwd[col, at_rows, :]
            prod = gn * cen[col, at_rows, :]
            out_sums.append(gsums[col] + prod[0:8] + prod[8:16])
            gain = gains[:, ln]
            gc = gn * gain
            fwd[col, at_rows, :] = gc
            prod = prod * gain
            one = gc if one is None else one + gc
            two = prod if two is None else two + prod
        sum1[at_rows, :] = one
        sum2[at_rows, :] = two
        return out_sums

    gsums = lax.fori_loop(0, SEG, grad_block, [jnp.zeros((8, 128), F32)] * NSP)
    for col in range(NSP):
        gkp[col, TAPS : TAPS + 1, :] = jnp.sum(gsums[col], axis=0, keepdims=True)
    m1 = jnp.sum(sum1[...], axis=1, keepdims=True) * (1.0 / D)
    m2 = jnp.sum(sum2[...], axis=1, keepdims=True) * (1.0 / D)
    sum1[...] = jnp.broadcast_to(m1, (ROWS, 128))
    sum2[...] = jnp.broadcast_to(m2, (ROWS, 128))

    def norm_block(j):
        at_rows = rows(j, 16)
        a, b, iv = sum1[at_rows, :], sum2[at_rows, :], inv_b[at_rows, :]
        for col in range(NSP):
            v = ((fwd[col, at_rows, :] - a - cen[col, at_rows, :] * b) * iv).astype(BF16)
            later[col, at_rows, :] = v
            gcp[at_rows, pl.ds(128 * col, 128)] = v

    loop(SEG, norm_block)

    def in_order(n):
        block = jnp.dot(perm[...], gcp[:, lanes(n, 1024)], preferred_element_type=F32)
        gcraw[0:ROWS, lanes(n, 1024)] = block.astype(BF16)

    loop(2, in_order)

    def margin_copy():
        return copy(
            gcraw.at[pl.ds(0, 32)], gcraw.at[pl.ds(ROWS, 32)], GC0, {"sp": (s + NSP - 1) % NSP, "dp": d}
        )

    @pl.when(s > 0)
    def _():
        margin_copy().start()

    def tap_block(col):
        grads, tiles, sums = later.at[col], ext.at[col], gkp.at[col]
        for k0 in range(0, TAPS, 4):
            taps_here = range(k0, min(k0 + 4, TAPS))
            acc = {}
            for j in range(SEG):
                for k in taps_here:
                    at_row = 16 * (j - k + 2 * SEG)
                    term = grads[16 * j : 16 * j + 16, :].astype(F32) * tiles[at_row : at_row + 16, :].astype(F32)
                    acc[k] = term if j == 0 else acc[k] + term
            for k in taps_here:
                sums[k : k + 1, :] = jnp.sum(acc[k][0:8] + acc[k][8:16], axis=0, keepdims=True)

    loop(NSP, tap_block)

    def send_gk(r):
        dst = (s + r + 1) % NSP
        copy(gkp.at[dst], gkr.at[r], GK0 + r, {"sp": dst, "dp": d}).start()

    loop(NSP - 1, send_gk)

    def stage1(c, h):
        pair = ((4, 3), (2, 5))[h]
        for n in pair:
            got(r1s[c].at[n], RA0 + 6 * c + n)
        own, cut = half_of(c, 0, h), (firsts, lasts)[h]
        dst = s1s[c].at[cut] if c == 1 else s1s[c].at[:, cut]

        def add(a, b):
            dst[a, b] = (
                own[a, b].astype(F32) + r1s[c][pair[0], a, b].astype(F32) + r1s[c][pair[1], a, b].astype(F32)
            ).astype(BF16)

        each(c, add)
        axis = (c + 1) % 3
        for r in (2, 1, 3):
            i = slot(axis, r)
            if c != 1:
                send(s1s[c].at[i, cut], r2s[c].at[r - 1, cut], RB0 + 6 * c + 2 * (r - 1) + h, at(axis, r))
            elif i // 2 == h:
                send(s1s[c].at[i], r2s[c].at[r - 1], RB0 + 6 * c + 2 * (r - 1), at(axis, r))

    def stage2(c):
        axis, last = (c + 1) % 3, (c + 2) % 3
        for r in range(1, 4):
            if c == 1:
                got(r2s[c].at[r - 1], RB0 + 6 * c + 2 * (r - 1))
            else:
                for h, cut in enumerate((firsts, lasts)):
                    got(r2s[c].at[r - 1, cut], RB0 + 6 * c + 2 * (r - 1) + h)

        def add(i):
            total = s1s[c][slot(axis, 0), i].astype(F32)
            for r in range(3):
                total = total + r2s[c][r, i].astype(F32)
            s2s[c][i] = total.astype(BF16)

        loop(4, add)
        for r in (2, 1, 3):
            for other in range(2):
                core = 1 - q if other else q
                send(
                    s2s[c].at[slot(last, r), rows(core, 16)],
                    r3s[c].at[other, r],
                    RC0 + 7 * c + 2 * r + other - 1,
                    at(last, r, core),
                )
        send(s2s[c].at[slot(last, 0), rows(1 - q, 16)], r3s[c].at[1, 0], RC0 + 7 * c, partner)

    factor = float(NSP * NDP * ROWS) ** (-0.5)

    def stage3(c):
        last = (c + 2) % 3
        first, size = COLOURS[c]
        got(r3s[c].at[1, 0], RC0 + 7 * c)
        for r in range(1, 4):
            for other in range(2):
                got(r3s[c].at[other, r], RC0 + 7 * c + 2 * r + other - 1)
        for other in range(2):
            if other:
                total = r3s[c][1, 0].astype(F32)
            else:
                total = s2s[c][slot(last, 0), rows(q, 16), :].astype(F32)
            for r in range(1, 4):
                total = total + r3s[c][other, r].astype(F32)
            core = 1 - q if other else q
            ow_ref[:, pl.ds(pl.multiple_of(core * HALF + first, 128), size)] = total * factor

    for c in (1, 0, 2):
        for h in range(2):
            stage1(c, h)

    @pl.when(s < NSP - 1)
    def _():
        got(gcraw.at[pl.ds(ROWS, 32)], GC0)

    @pl.when(s == NSP - 1)
    def _():
        gcraw[ROWS : ROWS + 32, :] = jnp.zeros((32, D), BF16)

    spread(gcraw, 16, later, ROWS)
    spread(gcraw, 32, later, 2 * ROWS)

    def back_block(col):
        ln = lanes(col)

        def emit(j, v):
            ggp[16 * j : 16 * j + 16, ln] = v.astype(BF16)

        filtered(col, later, lambda j, k: j + k, emit)

    out = []

    def finish(g):
        cols = pl.ds(512 * g, 512)
        grad = jnp.dot(perm[...], ggp[:, cols], preferred_element_type=F32)
        sg = sig[:, cols]
        gvo[:, cols] = (grad * sg).astype(BF16)
        ggo[:, cols] = (grad * val[:, cols].astype(F32) * sg * (1.0 - sg)).astype(BF16)
        for c in (
            pltpu.make_async_copy(gvo.at[:, cols], gv_hbm.at[:, cols], lsem.at[4 + 2 * g]),
            pltpu.make_async_copy(ggo.at[:, cols], gg_hbm.at[:, cols], lsem.at[5 + 2 * g]),
        ):
            c.start()
            out.append(c)

    def group(g):
        loop(4, lambda i: back_block(i + 4 * g))
        finish(g)

    group(0)

    group(1)
    def got_gk(r):
        got(gkr.at[r], GK0 + r)

    loop(NSP - 1, got_gk)
    total = gkp[s]
    for r in range(NSP - 1):
        total = total + gkr[r]
    gdo[...] = total

    def send_gd(r):
        copy(gdo, gdr.at[r], GD0 + r, {"sp": s, "dp": (d + r + 1) % NDP}).start()

    loop(NDP - 1, send_gd)
    group(2)
    group(3)
    for c in (1, 0, 2):
        stage2(c)
    for c in (1, 0, 2):
        stage3(c)

    def got_gd(r):
        got(gdr.at[r], GD0 + r)

    loop(NDP - 1, got_gd)
    total = gdo[...]
    for r in range(NDP - 1):
        total = total + gdr[r]
    gk_ref[...] = total * factor

    for c in sent:
        c.wait_send()

    def drain_sp(r):
        copy(tkall.at[s], tkall.at[s], TAP0 + r, partner).wait_send()
        copy(gkp.at[s], gkr.at[r], GK0 + r, partner).wait_send()

    loop(NSP - 1, drain_sp)

    def drain_dp(r):
        copy(gdo, gdr.at[r], GD0 + r, partner).wait_send()

    loop(NDP - 1, drain_dp)

    @pl.when(s < NSP - 1)
    def _():
        halo_copy(0).wait_send()
        halo_copy(1).wait_send()

    @pl.when(s > 0)
    def _():
        margin_copy().wait_send()

    for c in out:
        c.wait()


def place(gv_in, gg_in, ow_in, gk_in, gv_hbm, gg_hbm, ow_hbm, taps_hbm, gain_hbm, gv, gg, ow, gk, tp, gn, lsem, ssem):
    ins, outs = [], []
    for i in range(4):
        at_rows = pl.ds(64 * i, 64)
        ins.append(pltpu.make_async_copy(gv_in.at[at_rows], gv.at[at_rows], lsem.at[2 * i]))
        outs.append(pltpu.make_async_copy(gv.at[at_rows], gv_hbm.at[at_rows], ssem.at[2 * i]))
        ins.append(pltpu.make_async_copy(gg_in.at[at_rows], gg.at[at_rows], lsem.at[2 * i + 1]))
        outs.append(pltpu.make_async_copy(gg.at[at_rows], gg_hbm.at[at_rows], ssem.at[2 * i + 1]))
    ins.append(pltpu.make_async_copy(ow_in, ow, lsem.at[8]))
    outs.append(pltpu.make_async_copy(ow, ow_hbm, ssem.at[8]))
    small = pltpu.make_async_copy(gk_in, gk, lsem.at[9])
    small.start()
    for c in ins:
        c.start()
    for c, o in zip(ins, outs):
        c.wait()
        o.start()
    small.wait()
    tp[...] = gk[0:TAPS, :]
    gn[...] = gk[TAPS : TAPS + 1, :]
    outs.append(pltpu.make_async_copy(tp, taps_hbm, ssem.at[9]))
    outs.append(pltpu.make_async_copy(gn, gain_hbm, ssem.at[10]))
    outs[-2].start()
    outs[-1].start()
    for o in outs:
        o.wait()


def shards(out_cotangent, value_pre, gate_pre, out_weight, conv_kernel, norm_gain):
    hbm = pl.BlockSpec(memory_space=pl.ANY)
    vmem = pl.BlockSpec(memory_space=pltpu.VMEM)
    sizes = [size for _, size in COLOURS]
    scratch = [
        ((2, ROWS, D), BF16),
        ((2 * ROWS, D), BF16),
        ((ROWS, D), BF16),
        ((ROWS, D), BF16),
        ((ROWS, D), F32),
        ((ROWS + 32, D), BF16),
        ((NSP, 3 * ROWS, 128), BF16),
        ((NSP, ROWS, 128), F32),
        ((NSP, ROWS, 128), F32),
        ((2 * ROWS, D), BF16),
        ((4, ROWS, D), BF16),
        ((8, ROWS, ROWS), BF16),
        ((32, 128), F32),
        ((NSP, 32, 128), BF16),
        ((NSP, 16 * TAPS, 128), BF16),
        ((16, D), F32),
        ((ROWS, 128), F32),
        ((ROWS, 128), F32),
        ((ROWS, 128), F32),
        ((NSP, 3 * ROWS, 128), BF16),
        ((ROWS, D), BF16),
        ((ROWS + 32, D), BF16),
        ((ROWS, D), BF16),
        ((ROWS, D), BF16),
        ((ROWS, D), BF16),
        ((NSP, 32, 128), F32),
        ((NSP - 1, 32, 128), F32),
        ((32, 128), F32),
        ((NDP - 1, 32, 128), F32),
    ]
    scratch += [((4, 4, 4, 32, f), BF16) for f in sizes]
    halves = [(4, 2), (2, 4), (4, 2)]
    scratch += [((6, *h, 32, f), BF16) for h, f in zip(halves, sizes)]
    scratch += [((2, *h, 32, f), BF16) for h, f in zip(halves, sizes)]
    scratch += [((4, 4, 32, f), BF16) for f in sizes]
    scratch += [((3, 4, 32, f), BF16) for f in sizes]
    scratch += [((4, 32, f), BF16) for f in sizes]
    scratch += [((2, 4, 16, f), BF16) for f in sizes]
    scratch += [
        ((4, 2 * ROWS, ROWS), BF16),
        ((ROWS, ROWS), BF16),
        ((TAPS, 128), BF16),
        ((1, 128), BF16),
    ]
    grad_value, grad_gate, grad_weight, grad_taps = pl.pallas_call(
        kernel,
        out_shape=(
            jax.ShapeDtypeStruct((ROWS, D), BF16),
            jax.ShapeDtypeStruct((ROWS, D), BF16),
            jax.ShapeDtypeStruct((16, D), F32),
            jax.ShapeDtypeStruct((32, 128), F32),
        ),
        in_specs=[pl.BlockSpec(memory_space=pltpu.HBM)] * 6,
        out_specs=(hbm, hbm, vmem, vmem),
        scratch_shapes=[pltpu.VMEM(shape, kind) for shape, kind in scratch]
        + [pltpu.SemaphoreType.DMA((NSEM,)), pltpu.SemaphoreType.DMA((NSEM,)), pltpu.SemaphoreType.DMA((14,))],
        compiler_params=pltpu.CompilerParams(
            collective_id=0, has_side_effects=True, vmem_limit_bytes=60 * 1024 * 1024
        ),
    )(out_cotangent[0], value_pre[0], gate_pre[0], out_weight, conv_kernel, norm_gain[None])
    grad_value, grad_gate, grad_weight, grad_kernel, grad_gain = pl.pallas_call(
        place,
        out_shape=(
            jax.ShapeDtypeStruct((ROWS, D), BF16),
            jax.ShapeDtypeStruct((ROWS, D), BF16),
            jax.ShapeDtypeStruct((16, D), F32),
            jax.ShapeDtypeStruct((TAPS, 128), F32),
            jax.ShapeDtypeStruct((1, 128), F32),
        ),
        in_specs=[hbm] * 4,
        out_specs=(hbm,) * 5,
        scratch_shapes=[
            pltpu.VMEM((ROWS, D), BF16),
            pltpu.VMEM((ROWS, D), BF16),
            pltpu.VMEM((16, D), F32),
            pltpu.VMEM((32, 128), F32),
            pltpu.VMEM((TAPS, 128), F32),
            pltpu.VMEM((1, 128), F32),
            pltpu.SemaphoreType.DMA((10,)),
            pltpu.SemaphoreType.DMA((11,)),
        ],
    )(grad_value, grad_gate, grad_weight, grad_taps)
    return (grad_value[None], grad_gate[None], grad_weight, grad_kernel, grad_gain[0])


def solution(mesh):
    placed = (
        P("dp", "sp", None),
        P("dp", "sp", None),
        P("dp", "sp", None),
        P("dp", None),
        P(None, "sp"),
        P("sp"),
    )
    return jax.shard_map(
        shards,
        mesh=mesh,
        in_specs=placed,
        out_specs=(
            P("dp", "sp", None),
            P("dp", "sp", None),
            P(("sp", "dp"), None),
            P(None, "sp"),
            P("sp"),
        ),
        check_vma=False,
    )
```

```python
import functools

import jax
import jax.numpy as jnp
from jax import lax
from jax.experimental import pallas as pl
from jax.experimental.pallas import tpu as pltpu
from jax.sharding import PartitionSpec as P

EPS = 1e-05
F32 = jnp.float32
BF16 = jnp.bfloat16
MESH = pl.DeviceIdType.MESH

ROWS = 256
SEG = 16
D = 2048
HALF = 1024
TAPS = 31
NSP = 16
NDP = 8
WX_COLS, WY_COLS, WZ_COLS = (0, 384), (384, 896), (1280, 768)
COLOURS = ((0, 384), (384, 256), (640, 384))

TAP0 = 0
COT0 = TAP0 + 16
HALO0 = COT0 + 1
WX0 = HALO0 + 2
WY0 = WX0 + 12
WZ0 = WY0 + 12
ACT0 = WZ0 + 12
GA0 = ACT0 + 4
RA0 = GA0 + 4
RB0 = RA0 + 18
RC0 = RB0 + 18
GK0 = RC0 + 21
GD0 = GK0 + 16
GC0 = GD0 + 8
NSEM = GC0 + 1


def sigmoid(x):
    return 0.5 * jnp.tanh(0.5 * x) + 0.5


def lanes(i, n=128):
    return pl.ds(pl.multiple_of(i * n, n), n)


def rows(i, n):
    return pl.ds(pl.multiple_of(i * n, n), n)


def loop(n, body):
    def step(i, c):
        body(i)
        return c

    lax.fori_loop(0, n, step, 0)


def kernel(
    cot_hbm,
    val_hbm,
    gate_hbm,
    w_hbm,
    taps_hbm,
    gain_hbm,
    gv_hbm,
    gg_hbm,
    ow_ref,
    gk_ref,
    cotraw,
    cotp,
    val,
    gate,
    sig,
    gext,
    ext,
    cen,
    fwd,
    act,
    wg,
    ga,
    tkown,
    tkall,
    taps,
    gains,
    sum1,
    sum2,
    inv_b,
    later,
    gcp,
    gcraw,
    ggp,
    gvo,
    ggo,
    gkp,
    gkr,
    gdo,
    gdr,
    pa,
    pb,
    pc,
    r1a,
    r1b,
    r1c,
    cba,
    cbb,
    cbc,
    s1a,
    s1b,
    s1c,
    r2a,
    r2b,
    r2c,
    s2a,
    s2b,
    s2c,
    r3a,
    r3b,
    r3c,
    finp,
    perm,
    taps_in,
    gain_in,
    ssem,
    rsem,
    lsem,
):
    s = lax.axis_index("sp")
    d = lax.axis_index("dp")
    z, y = s // 4, s % 4
    x, q = d // 2, d % 2

    def at(axis, off, core=None):
        dp = d if core is None else x * 2 + core
        if axis == 0:
            return {"sp": s, "dp": ((x + off) % 4) * 2 + (q if core is None else core)}
        if axis == 1:
            return {"sp": z * 4 + (y + off) % 4, "dp": dp}
        return {"sp": ((z + off) % 4) * 4 + y, "dp": dp}

    def slot(axis, off):
        return (off - 1) % 4 if axis == 2 else (coord[axis] + off) % 4

    partner = {"sp": s, "dp": x * 2 + (1 - q)}
    coord = (x, y, z)

    sent = []

    def copy(src, dst, i, dev):
        return pltpu.make_async_remote_copy(
            src_ref=src, dst_ref=dst, send_sem=ssem.at[i], recv_sem=rsem.at[i], device_id=dev, device_id_type=MESH
        )

    def send(src, dst, i, dev):
        c = copy(src, dst, i, dev)
        c.start()
        sent.append(c)

    def got(dst, i):
        copy(dst, dst, i, partner).wait_recv()

    local = [
        pltpu.make_async_copy(w_hbm, wg.at[x], lsem.at[0]),
        pltpu.make_async_copy(val_hbm, val, lsem.at[1]),
        pltpu.make_async_copy(gate_hbm, gate, lsem.at[2]),
        pltpu.make_async_copy(cot_hbm, cotraw.at[q], lsem.at[3]),
    ]
    small = [
        pltpu.make_async_copy(taps_hbm, taps_in, lsem.at[12]),
        pltpu.make_async_copy(gain_hbm, gain_in, lsem.at[13]),
    ]
    for c in (local[0], *small, *local[1:]):
        c.start()
    barrier = pltpu.get_barrier_semaphore()

    def greet_sp(r):
        pl.semaphore_signal(barrier, inc=1, device_id={"sp": (s + r + 1) % NSP, "dp": d}, device_id_type=MESH)

    def greet_dp(r):
        pl.semaphore_signal(barrier, inc=1, device_id={"sp": s, "dp": (d + r + 1) % NDP}, device_id_type=MESH)

    loop(NSP - 1, greet_sp)
    loop(NDP - 1, greet_dp)
    for axis in (1, 2):
        for r in (1, 2, 3):
            pl.semaphore_signal(barrier, inc=1, device_id=at(axis, r, 1 - q), device_id_type=MESH)
    r_io = lax.broadcasted_iota(jnp.int32, (ROWS, ROWS), 0)
    t_io = lax.broadcasted_iota(jnp.int32, (ROWS, ROWS), 1)
    perm[...] = jnp.where(t_io == (r_io & 15) * SEG + (r_io >> 4), 1.0, 0.0).astype(BF16)
    local[1].wait()
    local[2].wait()

    def gate_block(i):
        at_rows = rows(ROWS // 32 - 1 - i, 32)
        sg = sigmoid(gate[at_rows, :].astype(F32))
        sig[at_rows, :] = sg
        gext[pl.ds(pl.multiple_of((ROWS // 32 - i) * 32, 32), 32), :] = (val[at_rows, :].astype(F32) * sg).astype(BF16)

    gate_block(0)

    def halo_copy(n):
        cols = pl.ds(HALF * n, HALF)
        return copy(
            gext.at[pl.ds(ROWS, 32), cols],
            gext.at[pl.ds(0, 32), cols],
            HALO0 + n,
            {"sp": (s + 1) % NSP, "dp": d},
        )
    pl.semaphore_wait(barrier, NSP - 1 + NDP - 1 + 6)

    def piece(cols, size):
        def at_quarter(xx, quarter, h=None):
            n, first = (size, quarter * size) if h is None else (size // 2, quarter * size + h * (size // 2))
            return wg.at[xx, pl.ds(pl.multiple_of(first, n), n), pl.ds(*cols)]

        return at_quarter

    wx, wy, wz = piece(WX_COLS, ROWS), piece(WY_COLS, 64), piece(WZ_COLS, 64)

    local[0].wait()
    for i, off in ((0, 1), (1, -1)):
        send(wy(x, y), wy(x, y), WX0 + i, at(0, off))
    for i, off in ((0, 1), (1, -1)):
        send(wz(x, z), wz(x, z), WX0 + 2 + i, at(0, off))

    @pl.when(s < NSP - 1)
    def _():
        halo_copy(0).start()

    for c in small:
        c.wait()
    tkown[0:TAPS, :] = taps_in[...].astype(F32)
    tkown[TAPS : TAPS + 1, :] = gain_in[...].astype(F32)
    tkall[s] = tkown[...].astype(BF16)

    def send_taps(r):
        copy(tkall.at[s], tkall.at[s], TAP0 + r, {"sp": (s + r + 1) % NSP, "dp": d}).start()

    loop(NSP - 1, send_taps)

    @pl.when(s < NSP - 1)
    def _():
        halo_copy(1).start()

    local[3].wait()
    send(cotraw.at[q], cotraw.at[q], COT0, partner)
    loop(ROWS // 32 - 1, lambda i: gate_block(i + 1))

    left, right, far = (x + 3) % 4, (x + 1) % 4, (x + 2) % 4
    both = ((0, 1), (1, -1))

    def along_x(part, quarter, base):
        for i, off in both:
            src = (x - off) % 4
            got(part(src, quarter), WX0 + base + i)
            send(part(src, quarter, i), part(src, quarter, i), WX0 + 6 + base + i, at(0, off))

    def far_along_x(part, quarter, base):
        for i, _ in both:
            got(part(far, quarter, i), WX0 + 6 + base + i)

    def across(axis, xx, pos):
        part, here, base = ((wy, y, WY0), (wz, z, WZ0))[axis - 1]
        for i, off in both:
            send(part(xx, here), part(xx, here), base + 4 * pos + i, at(axis, off))

    def across_on(axis, xx, pos):
        part, here, base = ((wy, y, WY0), (wz, z, WZ0))[axis - 1]
        for i, off in both:
            quarter = (here - off) % 4
            got(part(xx, quarter), base + 4 * pos + i)
            send(part(xx, quarter, i), part(xx, quarter, i), base + 4 * pos + 2 + i, at(axis, off))

    def across_end(axis, xx, pos):
        part, here, base = ((wy, y, WY0), (wz, z, WZ0))[axis - 1]
        for i, _ in both:
            got(part(xx, (here + 2) % 4, i), base + 4 * pos + 2 + i)

    def weights_end(xx, pos):
        across_end(1, xx, pos)
        across_end(2, xx, pos)
        if pos == 2:
            far_along_x(wx, 0, 4)

    def spread_half(src, first, dst, base, n):
        block = jnp.dot(perm[...], src[pl.ds(first, ROWS), lanes(n, HALF)], preferred_element_type=F32)
        block = block.astype(BF16)
        for i in range(8):
            dst[n * 8 + i, pl.ds(base, ROWS), :] = block[:, 128 * i : 128 * i + 128]

    def spread(src, first, dst, base):
        loop(2, lambda n: spread_half(src, first, dst, base, n))

    spread(gext, 32, ext, 2 * ROWS)

    def spread_cot(core):
        def body(n):
            block = jnp.dot(perm[...], cotraw[core, :, lanes(n, 1024)], preferred_element_type=F32)
            cotp[rows(core, ROWS), lanes(n, 1024)] = block.astype(BF16)

        loop(2, body)

    spread_cot(q)
    got(cotraw.at[1 - q], COT0)
    spread_cot(1 - q)

    def halo_in(n):
        cols = pl.ds(HALF * n, HALF)

        @pl.when(s > 0)
        def _():
            got(gext.at[pl.ds(0, 32), cols], HALO0 + n)

        @pl.when(s == 0)
        def _():
            gext[0:32, cols] = jnp.zeros((32, HALF), BF16)

    def spread_before(n):
        spread_half(gext, 16, ext, ROWS, n)
        spread_half(gext, 0, ext, 0, n)

    def got_taps(r):
        src = (s + NSP - 1 - r) % NSP
        got(tkall.at[src], TAP0 + r)

    def widen(i):
        t = tkall[i].astype(F32)
        gains[:, lanes(i)] = jnp.broadcast_to(t[TAPS : TAPS + 1], (16, 128))
        for k in range(TAPS):
            taps[i, 16 * k : 16 * k + 16, :] = jnp.broadcast_to(t[k : k + 1], (16, 128)).astype(BF16)

    def filtered(col, src, shift, emit):
        tiles, weights = src.at[col], taps.at[col]
        for j0 in range(0, SEG, 4):
            acc = [None] * 4
            for k in range(TAPS):
                for o in range(4):
                    at_row = 16 * shift(j0 + o, k)
                    term = weights[16 * k : 16 * k + 16, :].astype(F32) * tiles[at_row : at_row + 16, :].astype(F32)
                    acc[o] = term if acc[o] is None else acc[o] + term
            for o in range(4):
                emit(j0 + o, acc[o])

    def conv_block(col):
        dst = cen.at[col]

        def emit(j, v):
            dst[16 * j : 16 * j + 16, :] = v

        filtered(col, ext, lambda j, k: j - k + 2 * SEG, emit)

    halo_in(0)
    spread_before(0)
    along_x(wy, y, 0)
    across(1, left, 0)
    across(1, right, 1)
    loop(NSP - 1, got_taps)
    loop(NSP, widen)
    loop(8, conv_block)
    along_x(wz, z, 2)
    across(2, left, 0)
    across(2, right, 1)
    for i, off in both:
        send(wx(x, 0), wx(x, 0), WX0 + 4 + i, at(0, off))
    halo_in(1)
    spread_before(1)
    loop(8, lambda i: conv_block(i + 8))


    def conv_sums(j):
        at_rows = rows(j, 16)
        one = two = None
        for col in range(NSP):
            v = cen[col, at_rows, :]
            one = v if one is None else one + v
            two = v * v if two is None else two + v * v
        sum1[at_rows, :] = one
        sum2[at_rows, :] = two

    loop(SEG, conv_sums)
    mean = jnp.sum(sum1[...], axis=1, keepdims=True) * (1.0 / D)
    var = jnp.sum(sum2[...], axis=1, keepdims=True) * (1.0 / D) - mean * mean
    sum1[...] = jnp.broadcast_to(mean, (ROWS, 128))
    inv_b[...] = jnp.broadcast_to(lax.rsqrt(var + EPS), (ROWS, 128))

    def act_block(g, j):
        at_rows = rows(j, 16)
        m, iv = sum1[at_rows, :], inv_b[at_rows, :]
        for i in range(4):
            col = 4 * g + i
            ln = lanes(col)
            centred = (cen[col, at_rows, :] - m) * iv
            cen[col, at_rows, :] = centred
            normed = centred * gains[:, ln]
            sg = sigmoid(normed)
            act[pl.ds(pl.multiple_of(q * ROWS + j * 16, 16), 16), ln] = (normed * sg).astype(BF16)
            fwd[col, at_rows, :] = sg * (1.0 + normed * (1.0 - sg))

    order = (1, 0, 2, 3)
    groups = [(z + 1 + zr) % 4 for zr in order]
    for pos, g in enumerate(groups):
        loop(SEG, lambda j, g=g: act_block(g, j))
        part = act.at[rows(q, ROWS), lanes(g, 512)]
        send(part, part, ACT0 + pos, partner)
        if pos == 2:
            far_along_x(wy, y, 0)
            across(1, far, 2)
        if pos == 3:
            across_on(1, left, 0)
            far_along_x(wz, z, 2)
            across(2, far, 2)

    blocks = (pa, pb, pc)
    half = lanes(q, HALF)

    def outer(g, zr):
        p = lax.dot_general(
            act[:, lanes(g, 512)], cotp[:, half], (((0,), (0,)), ((), ())), preferred_element_type=F32
        ).astype(BF16)
        for n in range(16):
            yy, xx = n // 4, n % 4
            part = p[32 * n : 32 * n + 32]
            pa[xx, yy, zr] = part[:, 0:384]
            pb[yy, zr, xx] = part[:, 384:640]
            pc[zr, xx, yy] = part[:, 640:1024]

    r1s, cbs = (r1a, r1b, r1c), (cba, cbb, cbc)
    s1s, r2s, s2s, r3s = (s1a, s1b, s1c), (r2a, r2b, r2c), (s2a, s2b, s2c), (r3a, r3b, r3c)
    firsts, lasts = pl.ds(0, 2), pl.ds(2, 2)

    def half_of(c, off, h):
        cut = (firsts, lasts)[h]
        if c == 1:
            return blocks[c].at[slot(c, off), cut]
        return blocks[c].at[slot(c, off), :, cut]

    def sums_far(c, h):
        send(half_of(c, 2, h), r1s[c].at[h], RA0 + 6 * c + h, at(c, (1, -1)[h]))

    def sums_alone(c, h):
        send(half_of(c, (-1, 1)[h], h), r1s[c].at[3 - h], RA0 + 6 * c + 3 - h, at(c, (-1, 1)[h]))

    for pos, (g, zr) in enumerate(zip(groups, order)):
        got(act.at[rows(1 - q, ROWS), lanes(g, 512)], ACT0 + pos)
        outer(g, zr)
        if pos == 1:
            across_on(2, left, 0)
            across_on(1, right, 1)
            sums_far(0, 0)
            sums_alone(0, 0)
        if pos == 2:
            across_on(2, right, 1)
        if pos == 3:
            along_x(wx, 0, 4)
            sums_far(0, 1)
            across_on(1, far, 2)
            sums_far(1, 0)
            sums_far(1, 1)
            across_on(2, far, 2)
            sums_far(2, 0)
            sums_far(2, 1)
            for c in (2, 1):
                sums_alone(c, 0)
                sums_alone(c, 1)
            sums_alone(0, 1)

    def each(c, body):
        loop(8, (lambda i: body(i // 4, i % 4)) if c == 1 else (lambda i: body(i // 2, i % 2)))

    def join(c, h):
        got(r1s[c].at[h], RA0 + 6 * c + h)
        own = half_of(c, (1, -1)[h], h)

        def add(a, b):
            cbs[c][h, a, b] = (own[a, b].astype(F32) + r1s[c][h, a, b].astype(F32)).astype(BF16)

        each(c, add)
        send(cbs[c].at[h], r1s[c].at[4 + h], RA0 + 6 * c + 4 + h, at(c, (1, -1)[h]))

    def back_send(pos, xx):
        blk = xx * 2 + q
        g = lax.dot_general(cotp[...], wg[xx], (((1,), (1,)), ((), ())), preferred_element_type=F32).astype(BF16)
        finp[pos] = g
        ga[blk] = finp[pos, rows(q, ROWS), :]
        send(finp.at[pos, rows(1 - q, ROWS)], ga.at[blk], GA0 + pos, partner)

    back_send(3, x)
    weights_end(left, 0)
    back_send(0, left)
    weights_end(right, 1)
    back_send(1, right)
    join(0, 0)
    weights_end(far, 2)
    back_send(2, far)

    join(1, 0)
    join(1, 1)
    join(2, 0)
    join(2, 1)
    join(0, 1)

    for pos, off in ((3, 0), (0, 3), (1, 1), (2, 2)):
        got(ga.at[((x + off) % 4) * 2 + 1 - q], GA0 + pos)

    def grad_block(j, gsums):
        at_rows = rows(j, 16)
        one = two = None
        out_sums = []
        for col in range(NSP):
            ln = pl.ds(128 * col, 128)
            gn = ga[col // 2, at_rows, pl.ds(128 * (col % 2), 128)].astype(F32) * fwd[col, at_rows, :]
            prod = gn * cen[col, at_rows, :]
            out_sums.append(gsums[col] + prod[0:8] + prod[8:16])
            gain = gains[:, ln]
            gc = gn * gain
            fwd[col, at_rows, :] = gc
            prod = prod * gain
            one = gc if one is None else one + gc
            two = prod if two is None else two + prod
        sum1[at_rows, :] = one
        sum2[at_rows, :] = two
        return out_sums

    gsums = lax.fori_loop(0, SEG, grad_block, [jnp.zeros((8, 128), F32)] * NSP)
    for col in range(NSP):
        gkp[col, TAPS : TAPS + 1, :] = jnp.sum(gsums[col], axis=0, keepdims=True)
    m1 = jnp.sum(sum1[...], axis=1, keepdims=True) * (1.0 / D)
    m2 = jnp.sum(sum2[...], axis=1, keepdims=True) * (1.0 / D)
    sum1[...] = jnp.broadcast_to(m1, (ROWS, 128))
    sum2[...] = jnp.broadcast_to(m2, (ROWS, 128))

    def norm_block(j):
        at_rows = rows(j, 16)
        a, b, iv = sum1[at_rows, :], sum2[at_rows, :], inv_b[at_rows, :]
        for col in range(NSP):
            v = ((fwd[col, at_rows, :] - a - cen[col, at_rows, :] * b) * iv).astype(BF16)
            later[col, at_rows, :] = v
            gcp[at_rows, pl.ds(128 * col, 128)] = v

    loop(SEG, norm_block)

    def in_order(n):
        block = jnp.dot(perm[...], gcp[:, lanes(n, 1024)], preferred_element_type=F32)
        gcraw[0:ROWS, lanes(n, 1024)] = block.astype(BF16)

    loop(2, in_order)

    def margin_copy():
        return copy(
            gcraw.at[pl.ds(0, 32)], gcraw.at[pl.ds(ROWS, 32)], GC0, {"sp": (s + NSP - 1) % NSP, "dp": d}
        )

    @pl.when(s > 0)
    def _():
        margin_copy().start()

    def tap_block(col):
        grads, tiles, sums = later.at[col], ext.at[col], gkp.at[col]
        for k0 in range(0, TAPS, 4):
            taps_here = range(k0, min(k0 + 4, TAPS))
            acc = {}
            for j in range(SEG):
                for k in taps_here:
                    at_row = 16 * (j - k + 2 * SEG)
                    term = grads[16 * j : 16 * j + 16, :].astype(F32) * tiles[at_row : at_row + 16, :].astype(F32)
                    acc[k] = term if j == 0 else acc[k] + term
            for k in taps_here:
                sums[k : k + 1, :] = jnp.sum(acc[k][0:8] + acc[k][8:16], axis=0, keepdims=True)

    loop(NSP, tap_block)

    def send_gk(r):
        dst = (s + r + 1) % NSP
        copy(gkp.at[dst], gkr.at[r], GK0 + r, {"sp": dst, "dp": d}).start()

    loop(NSP - 1, send_gk)

    def stage1(c, h):
        pair = ((4, 3), (2, 5))[h]
        for n in pair:
            got(r1s[c].at[n], RA0 + 6 * c + n)
        own, cut = half_of(c, 0, h), (firsts, lasts)[h]
        dst = s1s[c].at[cut] if c == 1 else s1s[c].at[:, cut]

        def add(a, b):
            dst[a, b] = (
                own[a, b].astype(F32) + r1s[c][pair[0], a, b].astype(F32) + r1s[c][pair[1], a, b].astype(F32)
            ).astype(BF16)

        each(c, add)
        axis = (c + 1) % 3
        for r in (2, 1, 3):
            i = slot(axis, r)
            if c != 1:
                send(s1s[c].at[i, cut], r2s[c].at[r - 1, cut], RB0 + 6 * c + 2 * (r - 1) + h, at(axis, r))
            elif i // 2 == h:
                send(s1s[c].at[i], r2s[c].at[r - 1], RB0 + 6 * c + 2 * (r - 1), at(axis, r))

    def stage2(c):
        axis, last = (c + 1) % 3, (c + 2) % 3
        for r in range(1, 4):
            if c == 1:
                got(r2s[c].at[r - 1], RB0 + 6 * c + 2 * (r - 1))
            else:
                for h, cut in enumerate((firsts, lasts)):
                    got(r2s[c].at[r - 1, cut], RB0 + 6 * c + 2 * (r - 1) + h)

        def add(i):
            total = s1s[c][slot(axis, 0), i].astype(F32)
            for r in range(3):
                total = total + r2s[c][r, i].astype(F32)
            s2s[c][i] = total.astype(BF16)

        loop(4, add)
        for r in (2, 1, 3):
            for other in range(2):
                core = 1 - q if other else q
                send(
                    s2s[c].at[slot(last, r), rows(core, 16)],
                    r3s[c].at[other, r],
                    RC0 + 7 * c + 2 * r + other - 1,
                    at(last, r, core),
                )
        send(s2s[c].at[slot(last, 0), rows(1 - q, 16)], r3s[c].at[1, 0], RC0 + 7 * c, partner)

    factor = float(NSP * NDP * ROWS) ** (-0.5)

    def stage3(c):
        last = (c + 2) % 3
        first, size = COLOURS[c]
        got(r3s[c].at[1, 0], RC0 + 7 * c)
        for r in range(1, 4):
            for other in range(2):
                got(r3s[c].at[other, r], RC0 + 7 * c + 2 * r + other - 1)
        for other in range(2):
            if other:
                total = r3s[c][1, 0].astype(F32)
            else:
                total = s2s[c][slot(last, 0), rows(q, 16), :].astype(F32)
            for r in range(1, 4):
                total = total + r3s[c][other, r].astype(F32)
            core = 1 - q if other else q
            ow_ref[:, pl.ds(pl.multiple_of(core * HALF + first, 128), size)] = total * factor

    for c in (1, 0, 2):
        for h in range(2):
            stage1(c, h)

    @pl.when(s < NSP - 1)
    def _():
        got(gcraw.at[pl.ds(ROWS, 32)], GC0)

    @pl.when(s == NSP - 1)
    def _():
        gcraw[ROWS : ROWS + 32, :] = jnp.zeros((32, D), BF16)

    spread(gcraw, 16, later, ROWS)
    spread(gcraw, 32, later, 2 * ROWS)

    def back_block(col):
        ln = lanes(col)

        def emit(j, v):
            ggp[16 * j : 16 * j + 16, ln] = v.astype(BF16)

        filtered(col, later, lambda j, k: j + k, emit)

    out = []

    def finish(g):
        cols = pl.ds(512 * g, 512)
        grad = jnp.dot(perm[...], ggp[:, cols], preferred_element_type=F32)
        sg = sig[:, cols]
        gvo[:, cols] = (grad * sg).astype(BF16)
        ggo[:, cols] = (grad * val[:, cols].astype(F32) * sg * (1.0 - sg)).astype(BF16)
        for c in (
            pltpu.make_async_copy(gvo.at[:, cols], gv_hbm.at[:, cols], lsem.at[4 + 2 * g]),
            pltpu.make_async_copy(ggo.at[:, cols], gg_hbm.at[:, cols], lsem.at[5 + 2 * g]),
        ):
            c.start()
            out.append(c)

    def group(g):
        loop(4, lambda i: back_block(i + 4 * g))
        finish(g)

    group(0)

    group(1)
    def got_gk(r):
        got(gkr.at[r], GK0 + r)

    loop(NSP - 1, got_gk)
    total = gkp[s]
    for r in range(NSP - 1):
        total = total + gkr[r]
    gdo[...] = total

    def send_gd(r):
        copy(gdo, gdr.at[r], GD0 + r, {"sp": s, "dp": (d + r + 1) % NDP}).start()

    loop(NDP - 1, send_gd)
    group(2)
    group(3)
    for c in (1, 0, 2):
        stage2(c)
    for c in (1, 0, 2):
        stage3(c)

    def got_gd(r):
        got(gdr.at[r], GD0 + r)

    loop(NDP - 1, got_gd)
    total = gdo[...]
    for r in range(NDP - 1):
        total = total + gdr[r]
    gk_ref[...] = total * factor

    for c in sent:
        c.wait_send()

    def drain_sp(r):
        copy(tkall.at[s], tkall.at[s], TAP0 + r, partner).wait_send()
        copy(gkp.at[s], gkr.at[r], GK0 + r, partner).wait_send()

    loop(NSP - 1, drain_sp)

    def drain_dp(r):
        copy(gdo, gdr.at[r], GD0 + r, partner).wait_send()

    loop(NDP - 1, drain_dp)

    @pl.when(s < NSP - 1)
    def _():
        halo_copy(0).wait_send()
        halo_copy(1).wait_send()

    @pl.when(s > 0)
    def _():
        margin_copy().wait_send()

    for c in out:
        c.wait()


def place(gv_in, gg_in, ow_in, gk_in, gv_hbm, gg_hbm, ow_hbm, taps_hbm, gain_hbm, gv, gg, ow, gk, tp, gn, lsem, ssem):
    ins, outs = [], []
    for i in range(4):
        at_rows = pl.ds(64 * i, 64)
        ins.append(pltpu.make_async_copy(gv_in.at[at_rows], gv.at[at_rows], lsem.at[2 * i]))
        outs.append(pltpu.make_async_copy(gv.at[at_rows], gv_hbm.at[at_rows], ssem.at[2 * i]))
        ins.append(pltpu.make_async_copy(gg_in.at[at_rows], gg.at[at_rows], lsem.at[2 * i + 1]))
        outs.append(pltpu.make_async_copy(gg.at[at_rows], gg_hbm.at[at_rows], ssem.at[2 * i + 1]))
    ins.append(pltpu.make_async_copy(ow_in, ow, lsem.at[8]))
    outs.append(pltpu.make_async_copy(ow, ow_hbm, ssem.at[8]))
    small = pltpu.make_async_copy(gk_in, gk, lsem.at[9])
    small.start()
    for c in ins:
        c.start()
    small.wait()
    tp[...] = gk[0:TAPS, :]
    gn[...] = gk[TAPS : TAPS + 1, :]
    tiny = [pltpu.make_async_copy(tp, taps_hbm, ssem.at[9]), pltpu.make_async_copy(gn, gain_hbm, ssem.at[10])]
    for o in tiny:
        o.start()
    for c, o in zip(ins, outs):
        c.wait()
        o.start()
    outs = outs + tiny
    for o in outs:
        o.wait()


def shards(out_cotangent, value_pre, gate_pre, out_weight, conv_kernel, norm_gain):
    hbm = pl.BlockSpec(memory_space=pl.ANY)
    vmem = pl.BlockSpec(memory_space=pltpu.VMEM)
    sizes = [size for _, size in COLOURS]
    scratch = [
        ((2, ROWS, D), BF16),
        ((2 * ROWS, D), BF16),
        ((ROWS, D), BF16),
        ((ROWS, D), BF16),
        ((ROWS, D), F32),
        ((ROWS + 32, D), BF16),
        ((NSP, 3 * ROWS, 128), BF16),
        ((NSP, ROWS, 128), F32),
        ((NSP, ROWS, 128), F32),
        ((2 * ROWS, D), BF16),
        ((4, ROWS, D), BF16),
        ((8, ROWS, ROWS), BF16),
        ((32, 128), F32),
        ((NSP, 32, 128), BF16),
        ((NSP, 16 * TAPS, 128), BF16),
        ((16, D), F32),
        ((ROWS, 128), F32),
        ((ROWS, 128), F32),
        ((ROWS, 128), F32),
        ((NSP, 3 * ROWS, 128), BF16),
        ((ROWS, D), BF16),
        ((ROWS + 32, D), BF16),
        ((ROWS, D), BF16),
        ((ROWS, D), BF16),
        ((ROWS, D), BF16),
        ((NSP, 32, 128), F32),
        ((NSP - 1, 32, 128), F32),
        ((32, 128), F32),
        ((NDP - 1, 32, 128), F32),
    ]
    scratch += [((4, 4, 4, 32, f), BF16) for f in sizes]
    halves = [(4, 2), (2, 4), (4, 2)]
    scratch += [((6, *h, 32, f), BF16) for h, f in zip(halves, sizes)]
    scratch += [((2, *h, 32, f), BF16) for h, f in zip(halves, sizes)]
    scratch += [((4, 4, 32, f), BF16) for f in sizes]
    scratch += [((3, 4, 32, f), BF16) for f in sizes]
    scratch += [((4, 32, f), BF16) for f in sizes]
    scratch += [((2, 4, 16, f), BF16) for f in sizes]
    scratch += [
        ((4, 2 * ROWS, ROWS), BF16),
        ((ROWS, ROWS), BF16),
        ((TAPS, 128), BF16),
        ((1, 128), BF16),
    ]
    grad_value, grad_gate, grad_weight, grad_taps = pl.pallas_call(
        kernel,
        out_shape=(
            jax.ShapeDtypeStruct((ROWS, D), BF16),
            jax.ShapeDtypeStruct((ROWS, D), BF16),
            jax.ShapeDtypeStruct((16, D), F32),
            jax.ShapeDtypeStruct((32, 128), F32),
        ),
        in_specs=[pl.BlockSpec(memory_space=pltpu.HBM)] * 6,
        out_specs=(hbm, hbm, vmem, vmem),
        scratch_shapes=[pltpu.VMEM(shape, kind) for shape, kind in scratch]
        + [pltpu.SemaphoreType.DMA((NSEM,)), pltpu.SemaphoreType.DMA((NSEM,)), pltpu.SemaphoreType.DMA((14,))],
        compiler_params=pltpu.CompilerParams(
            collective_id=0, has_side_effects=True, vmem_limit_bytes=60 * 1024 * 1024
        ),
    )(out_cotangent[0], value_pre[0], gate_pre[0], out_weight, conv_kernel, norm_gain[None])
    grad_value, grad_gate, grad_weight, grad_kernel, grad_gain = pl.pallas_call(
        place,
        out_shape=(
            jax.ShapeDtypeStruct((ROWS, D), BF16),
            jax.ShapeDtypeStruct((ROWS, D), BF16),
            jax.ShapeDtypeStruct((16, D), F32),
            jax.ShapeDtypeStruct((TAPS, 128), F32),
            jax.ShapeDtypeStruct((1, 128), F32),
        ),
        in_specs=[hbm] * 4,
        out_specs=(hbm,) * 5,
        scratch_shapes=[
            pltpu.VMEM((ROWS, D), BF16),
            pltpu.VMEM((ROWS, D), BF16),
            pltpu.VMEM((16, D), F32),
            pltpu.VMEM((32, 128), F32),
            pltpu.VMEM((TAPS, 128), F32),
            pltpu.VMEM((1, 128), F32),
            pltpu.SemaphoreType.DMA((10,)),
            pltpu.SemaphoreType.DMA((11,)),
        ],
    )(grad_value, grad_gate, grad_weight, grad_taps)
    return (grad_value[None], grad_gate[None], grad_weight, grad_kernel, grad_gain[0])


def solution(mesh):
    placed = (
        P("dp", "sp", None),
        P("dp", "sp", None),
        P("dp", "sp", None),
        P("dp", None),
        P(None, "sp"),
        P("sp"),
    )
    return jax.shard_map(
        shards,
        mesh=mesh,
        in_specs=placed,
        out_specs=(
            P("dp", "sp", None),
            P("dp", "sp", None),
            P(("sp", "dp"), None),
            P(None, "sp"),
            P("sp"),
        ),
        check_vma=False,
    )
```
